32 devices in a mesh: sp: 8 (over z, y), tp: 4 (over x, core).
Axes of the slice: x: 2, y: 2, z: 4, core: 2. Of those that a mesh axis runs over, the one named last changes fastest.
Arguments:
- expert_in: bfloat16 [1024, 2048], P('sp'), may hold values from -6 to 6
- out_cot: bfloat16 [1024, 2048], P('sp'), may hold values from -8 to 8
- route_ids: int32 [1024, 2], P('sp'), may hold values from 0 to 7, all different within a row; in each aligned block of 128 rows (0 to 127, 128 to 255, ...) at most 64 rows name the same one
- route_weights: float32 [1024, 2], P('sp'), may hold values from 0.1 to 1
- w_gate: bfloat16 [8, 2048, 1024], P('sp', None, 'tp'), may hold values from -0.125 to 0.125
- w_up: bfloat16 [8, 2048, 1024], P('sp', None, 'tp'), may hold values from -0.125 to 0.125
- w_down: bfloat16 [8, 1024, 2048], P('sp', 'tp'), may hold values from -0.1875 to 0.1875
- w_out: bfloat16 [2048, 1024], P(None, 'tp'), may hold values from -0.1875 to 0.1875
- mixed_heads: bfloat16 [1024, 1024], P('sp', 'tp'), may hold values from -6 to 6
- queries: bfloat16 [1024, 512], P('sp', 'tp'), may hold values from -0.5 to 0.5
- keys: bfloat16 [1024, 512], P('sp', 'tp'), may hold values from -0.3125 to 0.3125
- values: bfloat16 [1024, 1024], P('sp', 'tp'), may hold values from -6 to 6
- log_decay: float32 [1024, 512], P('sp', 'tp'), may hold values from -0.3 to 0
Outputs:
- grad_gate: float32 [8, 2048, 1024], P('sp', None, 'tp')
- grad_up: float32 [8, 2048, 1024], P('sp', None, 'tp')
- grad_down: float32 [8, 1024, 2048], P('sp', 'tp')
- grad_out_proj: float32 [2048, 1024], P('sp', 'tp')
- grad_queries: bfloat16 [1024, 512], P('sp', 'tp')
- grad_keys: bfloat16 [1024, 512], P('sp', 'tp')
- grad_values: bfloat16 [1024, 1024], P('sp', 'tp')
- grad_decay: float32 [1024, 512], P('sp', 'tp')
The draws below stay inside these ranges and needn't reach their ends.
Inputs may be any that keep to these rules, and one draw needn't show every extreme that they name: `route_ids`: in the rows of one device no expert is named more than 64 times, a bound that some block reaches.
All inputs are finite; a program needn't handle non-finite values.
Results may differ from the reference program's by a relative error of at most 0.015.
Values may be sent and summed in bfloat16 or wider, within the bound.
A program may use at most 128 MiB of HBM per device.

```python
import math
import jax
import jax.numpy as jnp
import numpy as np
from jax import lax

D = 2048
FF = 1024
HEADS = 4
DK = 128
DV = 256
BLK = 128
TOP_K = 2
TOK_DEV = 128
EXPERTS = 8
CAP = 64
TOKENS = 1024
N_SP = 8
N_TP = 4


def draw_log_decay(key, part):
    channels = HEADS * DK
    keys_list = jax.random.split(key, 5)
    slow_share = 0.5
    is_slow = jax.random.uniform(keys_list[0], (channels,), jnp.float32) < slow_share
    slow_rate = jax.random.uniform(keys_list[1], (channels,), jnp.float32, 0.1, 0.5) / TOKENS
    fast_rate = jax.random.uniform(keys_list[2], (channels,), jnp.float32, 0.05, 0.1)
    decay_rate = jnp.where(is_slow, slow_rate, fast_rate)
    span_factor = jnp.exp(jax.random.uniform(keys_list[3], (TOKENS // BLK, 1, 1), jnp.float32, -math.log(2.0), math.log(2.0)))
    roughness = jax.random.uniform(keys_list[4], (TOKENS // BLK, BLK, channels), jnp.float32, 0.5, 1.5)
    return (-(decay_rate * span_factor * roughness)).reshape(TOKENS, channels)


def with_spikes(drawn, key, source, target, parts, factor):
    owner, partner = [(jnp.arange(drawn.shape[dim]) // (drawn.shape[dim] // parts)).reshape([-1 if axis == dim else 1 for axis in range(drawn.ndim)]) for dim in (source, target)]
    chosen = jax.random.permutation(key, parts)[partner]
    strong = (owner == chosen) | (owner == (partner + parts // 2) % parts)
    return jnp.where(strong, factor * drawn, drawn)


def block_scale(own_key, dims, cuts, least, largest):
    level = 1.0
    for dim, parts in cuts:
        steps = jax.random.uniform(jax.random.fold_in(jax.random.fold_in(own_key, 6), dim), (parts,), jnp.float32, least / len(cuts), largest / len(cuts))
        level = level * jnp.repeat(jnp.exp(steps), dims[dim] // parts).reshape((-1,) + (1,) * (len(dims) - 1 - dim))
    return level


def shared_out(key, own, number, rows, count, top, most, lean):
    sequence = jax.random.permutation(key, count)
    heavy_load, ordinary = portions_of(count, rows * top, most, lean, True), portions_of(count, rows * top, most, lean, False)
    places = jnp.arange(count)

    def named(lengths, turn):
        used = int((lengths > 0).sum())
        fixed = max(1, used // 4)
        shifted = fixed + (places - fixed + turn * (used - fixed)) % max(1, count - fixed)
        return jnp.zeros((count,), jnp.int32).at[sequence[jnp.where(places < fixed, places, shifted)]].set(jnp.asarray(lengths, jnp.int32))

    lengths = jnp.where(number % 4 == 0, named(heavy_load, number // 4), named(ordinary, number - number // 4 - 1))
    mixed = jax.random.permutation(jax.random.fold_in(own, 3), count)
    source_of, sink = mixed[0:count // 2 * 2:2], mixed[1:count // 2 * 2:2]
    slack = jnp.minimum(lengths[source_of] - 1, most - lengths[sink]) // 2
    slack = jnp.where((source_of == sequence[0]) | (sink == sequence[0]) | (lengths[sink] == 0), 0, jnp.maximum(slack, 0))
    shifted = jax.random.randint(jax.random.fold_in(own, 4), (count // 2,), 0, 1 << 20) % (slack + 1)
    lengths = lengths.at[source_of].add(-shifted).at[sink].add(shifted)
    labels = jnp.searchsorted(jnp.cumsum(lengths), jnp.arange(rows * top), side="right").astype(jnp.int32)
    table = labels.reshape(top, rows).T
    table = table[jax.random.permutation(jax.random.fold_in(own, 1), rows)]
    turn = jax.random.randint(jax.random.fold_in(own, 2), (rows, 1), 0, top)
    return jnp.take_along_axis(table, (jnp.arange(top)[None, :] + turn) % top, axis=1)


def portions_of(amount, total, bound, skew, full):
    portions = [(1 << 20) // math.isqrt(grade ** skew) + 1 for grade in range(1, amount + 1)]
    largest = bound if full else min(bound, max(-(-total // amount), total * portions[0] // sum(portions)))
    least = 1 if total - largest >= amount - 1 else 0
    given, rest = [largest] + [least] * (amount - 1), total - largest - least * (amount - 1)
    while rest > 0:
        free = [i for i in range(1, amount) if given[i] < largest] or [i for i in range(1, amount) if given[i] < bound]
        pool, left = sum([portions[i] for i in free]), rest
        for i in free:
            more = min(bound - given[i], max(1, left * portions[i] // pool), rest)
            given[i] = given[i] + more
            rest = rest - more
    return np.array(given)


def normal_values(own_key, shape, deviation, reach, pieces=(), kind=jnp.bfloat16):
    entries = jax.random.normal(own_key, shape, jnp.float32) * deviation
    if len(pieces) > 0:
        entries = block_scale(own_key, shape, pieces, -0.22, 0.18) * entries
    return jnp.clip(entries, min=-reach, max=reach).astype(kind)


def gaussian_with(rng, extent, width, bound, pieces, heavy, kind=jnp.bfloat16):
    result = width * jax.random.normal(rng, extent, jnp.float32)
    if pieces:
        result = result * block_scale(rng, extent, pieces, -0.22, 0.18)
    return jnp.clip(with_spikes(result, jax.random.fold_in(rng, 3), *heavy), -bound, bound).astype(kind)


def setup_inputs(seed: int = 0) -> dict:
    arg_keys = jax.random.split(jax.random.key(seed), 14)
    expert_in = normal_values(arg_keys[0], (TOKENS, D), 1.0, 6.0, ((0, 8),))
    out_cot = gaussian_with(arg_keys[1], (TOKENS, D), 1.0, 8.0, ((0, 8),), (0, 1, 8, 2.0))
    route_ids_keys = jax.random.split(jax.random.fold_in(arg_keys[2], 1), TOKENS // TOK_DEV)
    route_ids_turns = jax.random.permutation(jax.random.fold_in(arg_keys[2], 3), TOKENS // TOK_DEV)
    route_ids = jax.vmap(lambda own, number: shared_out(jax.random.fold_in(arg_keys[2], 2), own, number, TOK_DEV, EXPERTS, TOP_K, CAP, 1))(route_ids_keys, route_ids_turns).reshape((TOKENS, TOP_K))
    route_weights = jnp.clip(0.1 + 0.9 * jax.random.uniform(arg_keys[3], (TOKENS, TOP_K), jnp.float32) ** block_scale(arg_keys[3], (TOKENS, TOP_K), ((0, 8),), -0.2, 0.2), 0.1, 1.0)
    w_gate = normal_values(arg_keys[4], (EXPERTS, D, FF), D ** -0.5, 0.125, ((0, 8), (2, 4)))
    w_up = normal_values(arg_keys[5], (EXPERTS, D, FF), D ** -0.5, 0.125, ((0, 8), (2, 4)))
    w_down = normal_values(arg_keys[6], (EXPERTS, FF, D), FF ** -0.5, 0.1875, ((0, 8), (1, 4)))
    w_out = normal_values(arg_keys[7], (D, HEADS * DV), (HEADS * DV) ** -0.5, 0.1875, ((1, 4),))
    mixed_heads = normal_values(arg_keys[8], (TOKENS, HEADS * DV), 1.0, 6.0, ((0, 8), (1, 4)))
    queries = normal_values(arg_keys[9], (TOKENS, HEADS * DK), 0.09, 0.5, ((0, 8), (1, 4)))
    keys = normal_values(arg_keys[10], (TOKENS, HEADS * DK), 0.05, 0.3125, ((0, 8), (1, 4)))
    values = normal_values(arg_keys[11], (TOKENS, HEADS * DV), 1.0, 6.0, ((0, 8), (1, 4)))
    log_decay = draw_log_decay(jax.random.fold_in(arg_keys[13], 71), 0)
    return dict(expert_in=expert_in, out_cot=out_cot, route_ids=route_ids, route_weights=route_weights, w_gate=w_gate, w_up=w_up, w_down=w_down, w_out=w_out, mixed_heads=mixed_heads, queries=queries, keys=keys, values=values, log_decay=log_decay)


exact_mode = lax.Precision.HIGHEST

def block_forward(query_blocks, key_blocks, value_blocks, decay_blocks, state_start):
    block_len = query_blocks.shape[1]
    cumulative = jnp.cumsum(decay_blocks, axis=1)
    block_sum = cumulative[:, -1]
    query_decayed = query_blocks * jnp.exp(cumulative)
    key_grown = key_blocks * jnp.exp(-cumulative)
    key_to_end = key_blocks * jnp.exp(block_sum[:, None] - cumulative)
    causal = jnp.tril(jnp.ones((block_len, block_len), dtype=bool))
    scores = jnp.einsum('nchd,nshd->nhcs', query_decayed, key_grown, precision=exact_mode)
    scores = jnp.where(causal, scores, 0.0)
    intra_out = jnp.einsum('nhcs,nshe->nche', scores, value_blocks, precision=exact_mode)

    def advance(state_now, block):
        query_part, key_part, value_part, sum_part = block
        carried = jnp.einsum('chd,hde->che', query_part, state_now, precision=exact_mode)
        state_now = state_now * jnp.exp(sum_part)[..., None] + jnp.einsum('chd,che->hde', key_part, value_part, precision=exact_mode)
        return (state_now, carried)
    final_state, carried_out = lax.scan(advance, state_start, (query_decayed, key_to_end, value_blocks, block_sum))
    return (intra_out + carried_out, final_state)

def slot_table(route_ids):
    flat_ids = route_ids.reshape(N_SP, TOK_DEV * TOP_K)
    onehot = (flat_ids[..., None] == jnp.arange(EXPERTS, dtype=jnp.int32)).astype(jnp.int32)
    slot_rank = lax.optimization_barrier(jnp.sum((jnp.cumsum(onehot, axis=1) - 1) * onehot, axis=2)).astype(jnp.int32)
    source = jnp.arange(N_SP, dtype=jnp.int32)[:, None]
    slot_index = (flat_ids * (N_SP * CAP) + source * CAP + slot_rank).astype(jnp.int32)
    assign = jnp.arange(TOKENS * TOP_K, dtype=jnp.int32)
    table = jnp.full((EXPERTS * N_SP * CAP,), TOKENS * TOP_K, jnp.int32).at[slot_index.reshape(-1)].set(assign)
    return table.reshape(EXPERTS, N_SP * CAP)

def reference(expert_in, out_cot, route_ids, route_weights, w_gate, w_up, w_down, w_out, mixed_heads, queries, keys, values, log_decay):
    table = slot_table(route_ids)
    flat_weights = route_weights.reshape(-1)

    def per_expert(accum, pack):
        owners, gate_w, up_w, down_w = pack
        is_live = owners < TOKENS * TOP_K
        owner_safe = jnp.where(is_live, owners, 0)
        owner_token = owner_safe // TOP_K
        x_rows = jnp.where(is_live[:, None], expert_in[owner_token], jnp.zeros((), jnp.bfloat16))
        slot_weight = jnp.where(is_live, flat_weights[owner_safe], 0.0)
        dy_rows = (slot_weight[:, None] * out_cot[owner_token].astype(jnp.float32)).astype(jnp.bfloat16)
        gate_pre = jnp.dot(x_rows, gate_w, preferred_element_type=jnp.float32)
        up_pre = jnp.dot(x_rows, up_w, preferred_element_type=jnp.float32)
        sigmoid_gate = jax.nn.sigmoid(gate_pre)
        hidden = (gate_pre * sigmoid_gate * up_pre).astype(jnp.bfloat16)
        hidden_cot = jnp.dot(dy_rows, down_w.T, preferred_element_type=jnp.float32)
        grad_down = jnp.dot(hidden.T, dy_rows, preferred_element_type=jnp.float32)
        gate_cot = (hidden_cot * up_pre * sigmoid_gate * (1.0 + gate_pre * (1.0 - sigmoid_gate))).astype(jnp.bfloat16)
        up_cot = (hidden_cot * gate_pre * sigmoid_gate).astype(jnp.bfloat16)
        grad_gate = jnp.dot(x_rows.T, gate_cot, preferred_element_type=jnp.float32)
        grad_up = jnp.dot(x_rows.T, up_cot, preferred_element_type=jnp.float32)
        part = FF // N_TP
        rows_count = owners.shape[0]
        partial_value = jnp.einsum('snf,dnf->nsd', gate_cot.astype(jnp.float32).reshape(rows_count, N_TP, part), gate_w.astype(jnp.float32).reshape(D, N_TP, part))
        partial_value = partial_value + jnp.einsum('snf,dnf->nsd', up_cot.astype(jnp.float32).reshape(rows_count, N_TP, part), up_w.astype(jnp.float32).reshape(D, N_TP, part))
        input_cot = lax.optimization_barrier(jnp.sum(partial_value.astype(jnp.bfloat16).astype(jnp.float32), axis=0)).astype(jnp.bfloat16)
        accum = accum.at[owner_token].add(jnp.where(is_live[:, None], input_cot.astype(jnp.float32), 0.0))
        return (accum, (grad_gate, grad_up, grad_down))
    accum = jnp.zeros((TOKENS, D), jnp.float32)
    accum, (grad_gate, grad_up, grad_down) = lax.scan(per_expert, accum, (table, w_gate, w_up, w_down))
    mid_cot = (out_cot.astype(jnp.float32) + accum).astype(jnp.bfloat16)
    grad_out_proj = jnp.dot(mid_cot.T, mixed_heads, preferred_element_type=jnp.float32)
    head_cot = jnp.dot(mid_cot, w_out, preferred_element_type=jnp.float32)

    def mechanism(query_in, key_in, value_in, decay_in):
        blocks = TOKENS // BLK
        out, _ = block_forward(query_in.astype(jnp.float32).reshape(blocks, BLK, HEADS, DK), key_in.astype(jnp.float32).reshape(blocks, BLK, HEADS, DK), value_in.astype(jnp.float32).reshape(blocks, BLK, HEADS, DV), decay_in.reshape(blocks, BLK, HEADS, DK), jnp.zeros((HEADS, DK, DV), jnp.float32))
        return out.reshape(TOKENS, HEADS * DV)
    _, pull_back = jax.vjp(mechanism, queries, keys, values, log_decay)
    grad_queries, grad_keys, grad_values, grad_decay = pull_back(head_cot)
    return (grad_gate, grad_up, grad_down, grad_out_proj, grad_queries, grad_keys, grad_values, grad_decay)
```

```python
import functools

import jax
import jax.numpy as jnp
from jax import lax
from jax.experimental import pallas as pl
from jax.experimental.pallas import tpu as pltpu
from jax.sharding import PartitionSpec as P

DK = 128
EXACT = lax.Precision.HIGHEST
MESH = pl.DeviceIdType.MESH


def remote(src, dst, send, recv, device):
    return pltpu.make_async_remote_copy(
        src_ref=src, dst_ref=dst, send_sem=send, recv_sem=recv, device_id=device, device_id_type=MESH
    )


def greet(n_sp, me, tp, partners):
    barrier = pltpu.get_barrier_semaphore()

    def hello(i, carry):
        pl.semaphore_signal(
            barrier, inc=1, device_id=(lax.rem(me + i, n_sp), tp), device_id_type=MESH
        )
        return carry

    lax.fori_loop(1, n_sp, hello, 0)
    for other in partners:
        pl.semaphore_signal(barrier, inc=1, device_id=(me, other), device_id_type=MESH)
    pl.semaphore_wait(barrier, n_sp - 1 + len(partners))


def loop(start, stop, body):
    def step(i, carry):
        body(i)
        return carry

    lax.fori_loop(start, stop, step, 0)


def spread_kernel(n_sp, n_tp, n_rows, n_sides, *refs):
    count = n_rows + n_sides
    given, got = refs[:count], refs[count : 2 * count]
    s0, r0, s1, r1, s2, r2, s3, r3, s4, r4, own_sem = refs[2 * count :]
    me, tp = lax.axis_index("sp"), lax.axis_index("tp")
    far = lax.rem(tp + n_tp // 2, n_tp)
    near = tp + 1 - 2 * lax.rem(tp, 2)
    greet(n_sp, me, tp, (far, near))
    rows = tuple(zip(given[:n_rows], got[:n_rows]))
    sides = tuple(zip(given[n_rows:], got[n_rows:]))

    def first(j, p, slot):
        return remote(rows[j][0].at[p], rows[j][1].at[slot, tp], s0.at[j, p], r0.at[j, slot], (p, tp))

    def across(j, p, share):
        ref = rows[j][1].at[p, share]
        return remote(ref, ref, s1.at[j, p], r1.at[j, p], (me, far))

    def beside(j, p, share):
        ref = rows[j][1].at[p, share]
        return remote(ref, ref, s2.at[j, p], r2.at[j, p], (me, near))

    def relay(j, p, share):
        ref = rows[j][1].at[p, share]
        return remote(ref, ref, s3.at[j, p], r3.at[j, p], (me, near))

    def side(k, p, slot):
        return remote(sides[k][0], sides[k][1].at[slot], s4.at[k, p], r4.at[k, slot], (p, tp))

    def send(i):
        p = lax.rem(me + i, n_sp)
        for j in range(n_rows):
            first(j, p, me).start()

    loop(1, n_sp, send)
    owns = [
        pltpu.make_async_copy(rows[j][0].at[me], rows[j][1].at[me, tp], own_sem.at[j]) for j in range(n_rows)
    ] + [pltpu.make_async_copy(sides[k][0], sides[k][1].at[me], own_sem.at[n_rows + k]) for k in range(n_sides)]
    for own in owns:
        own.start()
    for own in owns:
        own.wait()
    for j in range(n_rows):
        across(j, me, tp).start()
        beside(j, me, tp).start()

    def send_side(i):
        p = lax.rem(me + i, n_sp)
        for k in range(n_sides):
            side(k, p, me).start()

    loop(1, n_sp, send_side)

    def forward(i):
        p = lax.rem(me - i + n_sp, n_sp)
        for j in range(n_rows):
            first(j, p, p).wait_recv()
            across(j, p, tp).start()
            beside(j, p, tp).start()

    loop(1, n_sp, forward)

    def pass_on(i):
        p = lax.rem(me - i + n_sp, n_sp)
        for j in range(n_rows):
            across(j, p, far).wait_recv()
            relay(j, p, far).start()

    loop(0, n_sp, pass_on)
    near_far = lax.rem(near + n_tp // 2, n_tp)

    def finish(i):
        p = lax.rem(me - i + n_sp, n_sp)
        for j in range(n_rows):
            beside(j, p, near).wait_recv()
            relay(j, p, near_far).wait_recv()
            across(j, p, tp).wait_send()
            beside(j, p, tp).wait_send()
            relay(j, p, far).wait_send()

    loop(0, n_sp, finish)

    def finish_side(i):
        p = lax.rem(me - i + n_sp, n_sp)
        for k in range(n_sides):
            side(k, p, p).wait_recv()
            side(k, p, me).wait_send()
        for j in range(n_rows):
            first(j, p, me).wait_send()

    loop(1, n_sp, finish_side)


def return_kernel(
    n_sp, n_tp, part, comb, dy, mix, state, mid, gmix, gstate, in1, out1, in2, out2, ret,
    s1, r1, s2, r2, s3, r3, s4, r4, s5, r5, own_sem,
):
    me, tp = lax.axis_index("sp"), lax.axis_index("tp")
    far = lax.rem(tp + n_tp // 2, n_tp)
    near = tp + 1 - 2 * lax.rem(tp, 2)
    near_far = lax.rem(near + n_tp // 2, n_tp)
    quarter = part.shape[2] // n_tp
    greet(n_sp, me, tp, (far, near))

    gathered = ((mix, gmix), (state, gstate))
    strides = [n_sp >> (k + 1) for k in range(n_sp.bit_length() - 1)]

    def hop(j, k, base, c):
        block = lax.rem(base, 2 * strides[k]) + c * 2 * strides[k]
        partner = me + strides[k] * (1 - 2 * lax.rem(me // strides[k], 2))
        ref = gathered[j][1].at[block]
        return remote(ref, ref, s5.at[j, k, c], r5.at[j, block], (partner, tp))

    def widen(k):
        def one(c):
            for j in (0, 1):
                hop(j, k, me, c).start()

        loop(0, n_sp // (2 * strides[k]), one)

    def arrive(k):
        partner = me + strides[k] * (1 - 2 * lax.rem(me // strides[k], 2))

        def one(c):
            for j in (0, 1):
                hop(j, k, partner, c).wait_recv()
                hop(j, k, me, c).wait_send()

        loop(0, n_sp // (2 * strides[k]), one)

    def columns(block):
        return pl.ds(pl.multiple_of(block * quarter, quarter), quarter)

    def beside(j, p):
        block = near if j == 0 else near_far
        return remote(
            part.at[p, :, columns(block)], in1.at[p, j], s1.at[j, p], r1.at[j, p], (me, near)
        )

    def across(p):
        return remote(out1.at[p], in2.at[p], s2.at[p], r2.at[p], (me, far))

    def back(p, slot):
        return remote(out2.at[p], ret.at[slot], s3.at[p], r3.at[slot], (p, tp))

    def start(i):
        p = lax.rem(me + 1 + i, n_sp)
        for j in (1, 0):
            beside(j, p).start()

    loop(0, n_sp, start)
    owns = [
        pltpu.make_async_copy(gathered[j][0], gathered[j][1].at[me], own_sem.at[j]) for j in (0, 1)
    ]
    for own in owns:
        own.start()
    for own in owns:
        own.wait()
    widen(0)

    def pair(i):
        p = lax.rem(me + 1 + i, n_sp)
        beside(1, p).wait_recv()
        mine = part[p, :, columns(far)].astype(jnp.float32)
        out1[p] = (mine + in1[p, 1].astype(jnp.float32)).astype(jnp.bfloat16)
        across(p).start()

    loop(0, n_sp, pair)
    arrive(0)
    for k in range(1, len(strides) - 1):
        widen(k)
        arrive(k)

    def total(p):
        beside(0, p).wait_recv()
        across(p).wait_recv()
        mine = part[p, :, columns(tp)].astype(jnp.float32)
        mine = mine + in1[p, 0].astype(jnp.float32)
        return (mine + in2[p].astype(jnp.float32)).astype(jnp.bfloat16)

    def quad(i):
        p = lax.rem(me + i, n_sp)
        out2[p] = total(p)
        back(p, me).start()

    loop(1, n_sp, quad)
    ret[me] = total(me)
    widen(len(strides) - 1)

    def gather(i, acc):
        p = lax.rem(me - i + n_sp, n_sp)

        @pl.when(i > 0)
        def _():
            back(p, p).wait_recv()

        return acc + jnp.dot(comb[p], ret[p], preferred_element_type=jnp.float32)

    acc = lax.fori_loop(0, n_sp, gather, dy[:, columns(tp)].astype(jnp.float32))
    mid[:, columns(tp)] = acc.astype(jnp.bfloat16)

    def share(k, block, device):
        ref = mid.at[:, columns(block)]
        return remote(ref, ref, s4.at[k], r4.at[k], (me, device))

    share(0, tp, far).start()
    share(1, tp, near).start()
    share(0, far, far).wait_recv()
    share(2, far, near).start()
    share(1, near, near).wait_recv()
    share(2, near_far, near).wait_recv()
    share(0, tp, far).wait_send()
    share(1, tp, near).wait_send()
    share(2, far, near).wait_send()

    arrive(len(strides) - 1)

    def finish(i):
        p = lax.rem(me + i, n_sp)
        for j in (0, 1):
            beside(j, p).wait_send()
        across(p).wait_send()

        @pl.when(i > 0)
        def _():
            back(p, me).wait_send()

    loop(0, n_sp, finish)


VM = pl.BlockSpec(memory_space=pltpu.VMEM)
ANY = pl.BlockSpec(memory_space=pl.ANY)


def dma(*shape):
    return [pltpu.SemaphoreType.DMA(shape), pltpu.SemaphoreType.DMA(shape)]


def call(kernel, ident, operands, in_specs, out_shape, out_specs, scratch):
    return pl.pallas_call(
        kernel,
        out_shape=out_shape,
        in_specs=in_specs,
        out_specs=out_specs,
        scratch_shapes=scratch,
        compiler_params=pltpu.CompilerParams(
            collective_id=ident, has_side_effects=True, vmem_limit_bytes=48 * 1024 * 1024
        ),
    )(*operands)


def spread_plan(
    expert_in, out_cot, route_ids, route_weights, w_gate, w_up, w_down, w_out,
    mixed_heads, queries, keys, values, log_decay,
):
    bf16, f32 = jnp.bfloat16, jnp.float32
    n_sp, n_tp = lax.axis_size("sp"), lax.axis_size("tp")
    me, tp = lax.axis_index("sp"), lax.axis_index("tp")
    tok, width = expert_in.shape
    top = route_ids.shape[1]
    experts = w_gate.shape[0] * n_sp
    cap = 2 * top * tok // experts
    share = cap // n_tp

    ids = route_ids.reshape(-1)
    onehot = ids[:, None] == jnp.arange(experts, dtype=jnp.int32)
    order = jnp.arange(tok * top, dtype=jnp.int32)
    below = (order[None, :] < order[:, None]).astype(bf16)
    ranks = jnp.dot(below, onehot.astype(bf16), preferred_element_type=f32)
    rank = jnp.sum(jnp.where(onehot, ranks, 0.0), axis=1).astype(jnp.int32)
    slot = (ids * cap + rank).reshape(tok, top)
    mine = (
        jnp.arange(experts, dtype=jnp.int32)[:, None] * cap
        + tp * share
        + jnp.arange(share, dtype=jnp.int32)[None, :]
    ).reshape(-1)
    match = slot[None] == mine[:, None, None]
    pick = jnp.any(match, axis=2).astype(bf16)
    slot_weight = jnp.sum(jnp.where(match, route_weights[None], 0.0), axis=(1, 2))
    x_share = jnp.dot(pick, expert_in, preferred_element_type=f32).astype(bf16)
    dy_share = (
        slot_weight[:, None] * jnp.dot(pick, out_cot, preferred_element_type=f32)
    ).astype(bf16)
    places = jnp.arange(experts * cap, dtype=jnp.int32).reshape(experts, 1, cap, 1)
    comb = jnp.any(slot[None, :, None, :] == places, axis=3).astype(bf16)

    heads = queries.shape[1] // DK
    dv = values.shape[1] // heads
    step = jnp.arange(tok, dtype=jnp.int32)
    causal = step[None, :] <= step[:, None]
    lower = causal.astype(f32)
    cumulative = jnp.dot(lower, log_decay, precision=EXACT)
    decay_sum = cumulative[-1:]

    def split(array):
        return array.astype(f32).reshape(tok, heads, -1)

    q, k, v = split(queries), split(keys), split(values)
    grow, shrink, to_end = (
        split(jnp.exp(-cumulative)),
        split(jnp.exp(cumulative)),
        split(jnp.exp(decay_sum - cumulative)),
    )
    qd, kg, ke = q * shrink, k * grow, k * to_end
    state_local = jnp.einsum("thd,the->hde", ke, v, precision=EXACT)

    rows = jax.ShapeDtypeStruct((n_sp, n_tp, share, width), bf16)
    gx, gdy, gdecay = call(
        functools.partial(spread_kernel, n_sp, n_tp, 2, 1),
        0,
        (
            x_share.reshape(n_sp, share, width),
            dy_share.reshape(n_sp, share, width),
            decay_sum,
        ),
        [VM] * 3,
        (
            rows,
            rows,
            jax.ShapeDtypeStruct((n_sp,) + decay_sum.shape, f32),
        ),
        (ANY, ANY, ANY),
        dma(2, n_sp) * 4 + dma(1, n_sp) + [pltpu.SemaphoreType.DMA((3,))],
    )
    got_x = gx.reshape(n_sp * cap, width)
    got_dy = gdy.reshape(n_sp * cap, width)
    wg, wu, wd = w_gate[0], w_up[0], w_down[0]
    gate_pre = jnp.dot(got_x, wg, preferred_element_type=f32)
    up_pre = jnp.dot(got_x, wu, preferred_element_type=f32)
    hidden_cot = lax.dot_general(got_dy, wd, (((1,), (1,)), ((), ())), preferred_element_type=f32)
    sig = jax.nn.sigmoid(gate_pre)
    hidden = (gate_pre * sig * up_pre).astype(bf16)
    gate_cot = (hidden_cot * up_pre * sig * (1.0 + gate_pre * (1.0 - sig))).astype(bf16)
    up_cot = (hidden_cot * gate_pre * sig).astype(bf16)
    back = (((1,), (1,)), ((), ()))
    part = lax.dot_general(gate_cot, wg, back, preferred_element_type=f32) + lax.dot_general(
        up_cot, wu, back, preferred_element_type=f32
    )
    part = part.astype(bf16).reshape(n_sp, cap, width)
    over = (((0,), (0,)), ((), ()))
    grad_gate = lax.dot_general(got_x, gate_cot, over, preferred_element_type=f32)[None]
    grad_up = lax.dot_general(got_x, up_cot, over, preferred_element_type=f32)[None]
    grad_down = lax.dot_general(hidden, got_dy, over, preferred_element_type=f32)[None]

    quarter = width // n_tp
    buf = pltpu.VMEM((n_sp, cap, quarter), bf16)
    mid, gmix, gstate = call(
        functools.partial(return_kernel, n_sp, n_tp),
        1,
        (part, comb, out_cot, mixed_heads, state_local.reshape(heads * DK, dv).astype(bf16)),
        [VM] * 5,
        (
            jax.ShapeDtypeStruct((tok, width), bf16),
            jax.ShapeDtypeStruct((n_sp,) + mixed_heads.shape, bf16),
            jax.ShapeDtypeStruct((n_sp, heads * DK, dv), bf16),
        ),
        (VM, VM, VM),
        [pltpu.VMEM((n_sp, 2, cap, quarter), bf16), buf, buf, buf, buf]
        + dma(2, n_sp) + dma(n_sp) + dma(n_sp) + dma(3)
        + [
            pltpu.SemaphoreType.DMA((2, n_sp.bit_length() - 1, n_sp // 2)),
            pltpu.SemaphoreType.DMA((2, n_sp)),
            pltpu.SemaphoreType.DMA((2,)),
        ],
    )
    head_cot = split(jnp.dot(mid, w_out, preferred_element_type=f32))
    pull = jnp.einsum("thd,the->hde", qd, head_cot, precision=EXACT)
    part_tok = tok // n_tp
    cols = lax.dynamic_slice_in_dim(mid, tp * part_tok, part_tok, 0)
    cols = cols.reshape(part_tok, n_sp, width // n_sp).swapaxes(0, 1)
    gcols, gpull = call(
        functools.partial(spread_kernel, n_sp, n_tp, 1, 1),
        2,
        (cols, pull.reshape(heads * DK, dv).astype(bf16)),
        [VM] * 2,
        (
            jax.ShapeDtypeStruct((n_sp, n_tp, part_tok, width // n_sp), bf16),
            jax.ShapeDtypeStruct((n_sp, heads * DK, dv), bf16),
        ),
        (VM, VM),
        dma(1, n_sp) * 5 + [pltpu.SemaphoreType.DMA((2,))],
    )
    gcols = gcols.reshape(n_sp, tok, width // n_sp)
    grad_out_proj = jnp.einsum("ntd,nte->de", gcols, gmix, preferred_element_type=f32)

    sums = gdecay[:, 0]
    index = jnp.arange(n_sp, dtype=jnp.int32)
    between = (index[None] > jnp.minimum(index, me)[:, None]) & (
        index[None] < jnp.maximum(index, me)[:, None]
    )
    weight = jnp.exp(jnp.sum(jnp.where(between[..., None], sums[None], 0.0), axis=1))

    def entering(pieces, used):
        scale = jnp.where(used[:, None], weight, 0.0)
        return jnp.sum(scale[..., None] * pieces.astype(f32), axis=0).reshape(heads, DK, dv)

    state_in = entering(gstate, index < me)
    state_cot = entering(gpull, index > me)

    dot = functools.partial(jnp.einsum, precision=EXACT)
    scores = jnp.where(causal, dot("thd,shd->hts", qd, kg), 0.0)
    scores_cot = jnp.where(causal, dot("the,she->hts", head_cot, v), 0.0)
    grad_v = dot("hts,the->she", scores, head_cot) + dot("shd,hde->she", ke, state_cot)
    qd_cot = dot("hts,shd->thd", scores_cot, kg) + dot("the,hde->thd", head_cot, state_in)
    kg_cot = dot("hts,thd->shd", scores_cot, qd)
    ke_cot = dot("she,hde->shd", v, state_cot)
    end = ke_cot * ke
    c_cot = (qd_cot * qd - kg_cot * kg - end).reshape(tok, heads * DK)
    last = jnp.sum(end, axis=0).reshape(-1) + jnp.exp(decay_sum[0]) * jnp.sum(
        state_cot * state_in, axis=2
    ).reshape(-1)
    grad_decay = lax.dot_general(lower, c_cot, over, precision=EXACT) + last[None]
    grad_q = (qd_cot * shrink).astype(bf16).reshape(tok, heads * DK)
    grad_k = (kg_cot * grow + ke_cot * to_end).astype(bf16).reshape(tok, heads * DK)
    return (
        grad_gate,
        grad_up,
        grad_down,
        grad_out_proj,
        grad_q,
        grad_k,
        grad_v.astype(bf16).reshape(tok, heads * dv),
        grad_decay,
    )


class Copies:
    def __init__(self, send, recv):
        self.send, self.recv = send, recv


def dot(a, b, dims, exact=False):
    return lax.dot_general(
        a, b, (dims, ((), ())), precision=EXACT if exact else None, preferred_element_type=jnp.float32
    )


NN, NT, TN = ((1,), (0,)), ((1,), (1,)), ((0,), (0,))


def whole_kernel(n_sp, n_tp, *refs):
    bf16, f32 = jnp.bfloat16, jnp.float32
    given, refs = refs[:13], refs[13:]
    outs, refs = refs[:8], refs[8:]
    x_hbm, dy_hbm, ids, weights, *_ = given
    grad_gate, grad_up, grad_down, grad_proj, grad_q, grad_k, grad_v, grad_decay = outs
    (
        x_in, dy_in, wg, wu, wd, wo, mixed, qv, kv, vv, gv,
        pos_t, wt, comb, xs, dys, gx, gdy, cots, hid, part, in1, out1, in2, out2, ret,
        mid, gmix, gcols, dall, fsend, frecv, usend, urecv, ftot, fpre, utot, upre,
        head, qd_s, kg_s, ke_s, sc_s, qc_s, kc_s, gv_s, cum_s,
        load, own_sem, *sems,
    ) = refs
    pairs = [Copies(a, b) for a, b in zip(sems[::2], sems[1::2])]
    (
        c_first, c_across, c_beside, c_relay, c_sum, c_mix, c_fwd, c_half, c_cross, c_back,
        c_share, c_rev, d_first, d_across, d_beside, d_relay,
    ) = pairs
    me, tp = lax.axis_index("sp"), lax.axis_index("tp")
    far = lax.rem(tp + n_tp // 2, n_tp)
    near = tp + 1 - 2 * lax.rem(tp, 2)
    near_far = lax.rem(near + n_tp // 2, n_tp)
    tok, width = x_in.shape
    share = xs.shape[1]
    cap = share * n_tp
    quarter = width // n_tp
    piece = width // n_sp
    rows = tok // n_tp
    bits = n_sp.bit_length() - 1

    sources = (x_hbm, dy_hbm) + tuple(given[4:])
    places = (x_in, dy_in, wg, wu, wd, wo, mixed, qv, kv, vv, gv)

    def fetch(i):
        src = sources[i].at[0] if len(sources[i].shape) == 3 else sources[i]
        return pltpu.make_async_copy(src, places[i], load.at[i])

    for i in range(len(places)):
        fetch(i).start()

    barrier = pltpu.get_barrier_semaphore()

    def hello(i):
        pl.semaphore_signal(
            barrier, inc=1, device_id=(lax.rem(me + i, n_sp), tp), device_id_type=MESH
        )

    loop(1, n_sp, hello)
    for other in (far, near):
        pl.semaphore_signal(barrier, inc=1, device_id=(me, other), device_id_type=MESH)

    def flip(m):
        out = 0
        for b in range(bits):
            a, c = lax.rem(me // (1 << b), 2), lax.rem(m // (1 << b), 2)
            out = out + (1 << b) * (a + c - 2 * a * c)
        return out

    def columns(block):
        return pl.ds(pl.multiple_of(block * quarter, quarter), quarter)

    lane = lax.broadcasted_iota(jnp.int32, (tok, 128), 1)
    down = lax.broadcasted_iota(jnp.int32, (tok, tok), 0)
    across_i = lax.broadcasted_iota(jnp.int32, (tok, tok), 1)
    first_hit = ids[:, 0:1] == lane
    weight = jnp.where(first_hit, weights[:, 0:1], 0.0)
    hit = jnp.where(first_hit, 1.0, 0.0)
    for j in range(1, ids.shape[1]):
        hit_j = ids[:, j : j + 1] == lane
        weight = weight + jnp.where(hit_j, weights[:, j : j + 1], 0.0)
        hit = hit + jnp.where(hit_j, 1.0, 0.0)
    below = jnp.where(across_i < down, 1.0, 0.0).astype(bf16)
    rank = dot(below, hit.astype(bf16), NN)
    pos = jnp.where(hit > 0.5, rank, -1.0)
    pos_t[...] = jnp.transpose(pos)
    wt[...] = jnp.transpose(weight)
    slot_lane = lax.broadcasted_iota(jnp.int32, (tok, cap), 1).astype(f32)
    for e in range(n_sp):
        comb[:, e * cap : (e + 1) * cap] = jnp.where(pos[:, e : e + 1] == slot_lane, 1.0, 0.0).astype(bf16)

    fetch(0).wait()
    fetch(1).wait()

    def chosen(e, start, count):
        want = (lax.broadcasted_iota(jnp.int32, (count, tok), 0) + start).astype(f32)
        match = pos_t[pl.ds(e, 1), :] == want
        scale = jnp.sum(jnp.where(match, wt[pl.ds(e, 1), :], 0.0), axis=1, keepdims=True)
        return jnp.where(match, 1.0, 0.0), scale

    found = [chosen(e, tp * share, share) for e in range(n_sp)]
    pick = jnp.concatenate([a for a, _ in found], axis=0).astype(bf16)
    scale = jnp.concatenate([b for _, b in found], axis=0)
    xs[...] = dot(pick, x_in[...], NN).astype(bf16).reshape(n_sp, share, width)
    dys[...] = (scale * dot(pick, dy_in[...], NN)).astype(bf16).reshape(n_sp, share, width)

    pl.semaphore_wait(barrier, n_sp + 1)

    row_pairs = ((xs, gx), (dys, gdy))

    def first(j, p, slot):
        return remote(
            row_pairs[j][0].at[p], row_pairs[j][1].at[slot, tp],
            c_first.send.at[j, p], c_first.recv.at[j, slot], (p, tp),
        )

    def passing(copies, j, p, block, device):
        ref = row_pairs[j][1].at[p, block]
        return remote(ref, ref, copies.send.at[j, p], copies.recv.at[j, p], (me, device))

    def across(j, p, block):
        return passing(c_across, j, p, block, far)

    def beside(j, p, block):
        return passing(c_beside, j, p, block, near)

    def relay(j, p, block):
        return passing(c_relay, j, p, block, near)

    def dispatch(m):
        p = flip(m)
        for j in (0, 1):
            first(j, p, me).start()

    loop(1, n_sp, dispatch)

    own_pick, own_scale = chosen(me, 0, cap)
    own_pick = own_pick.astype(bf16)
    gx[me] = dot(own_pick, x_in[...], NN).astype(bf16).reshape(n_tp, share, width)
    gdy[me] = (own_scale * dot(own_pick, dy_in[...], NN)).astype(bf16).reshape(n_tp, share, width)

    for i in range(6, 11):
        fetch(i).wait()
    causal = across_i <= down
    lower = jnp.where(causal, 1.0, 0.0)
    cum = dot(lower, gv[...], NN, True)
    total_decay = cum[tok - 1 : tok, :]
    cum_s[...] = cum
    dall[me] = jnp.broadcast_to(total_decay, dall.shape[1:])

    def decay(p, slot):
        return remote(dall.at[me], dall.at[slot], c_sum.send.at[p], c_sum.recv.at[slot], (p, tp))

    def send_decay(m):
        decay(flip(m), me).start()

    loop(1, n_sp, send_decay)
    key = kv[...].astype(f32)
    val = vv[...].astype(f32)
    qd_s[...] = qv[...].astype(f32) * jnp.exp(cum)
    kg_s[...] = key * jnp.exp(-cum)
    ke_s[...] = key * jnp.exp(total_decay - cum)
    ftot[...] = dot(val, ke_s[...], TN, True)
    fpre[...] = jnp.zeros_like(fpre)

    def hop(copies, held, got, k):
        partner = me + (1 << k) * (1 - 2 * lax.rem(me // (1 << k), 2))
        return remote(held.at[k], got.at[k], copies.send.at[k], copies.recv.at[k], (partner, tp))

    def give(copies, held, got, total, k):
        held[k] = total[...].astype(bf16)
        hop(copies, held, got, k).start()

    def decay_over(low, high):
        table = dall[:, 0, :]
        index = lax.broadcasted_iota(jnp.int32, table.shape, 0)
        picked = jnp.where((index >= low) & (index < high), table, 0.0)
        return jnp.exp(jnp.sum(picked, axis=0, keepdims=True))

    def span(k):
        size = 1 << k
        base = me - lax.rem(me, size)
        upper = lax.rem(me // size, 2)
        return base, base + size, upper

    def forward_merge(k):
        hop(c_fwd, fsend, frecv, k).wait_recv()
        low, high, upper = span(k)
        got = frecv[k].astype(f32)
        is_upper = upper == 1
        fpre[...] = fpre[...] + jnp.where(is_upper, decay_over(low, me), 0.0) * got
        mine = jnp.where(is_upper, 1.0, decay_over(low + (1 << k), high + (1 << k)))
        theirs = jnp.where(is_upper, decay_over(low, high), 1.0)
        ftot[...] = mine * ftot[...] + theirs * got

    def reverse_merge(k):
        hop(c_rev, usend, urecv, k).wait_recv()
        low, high, upper = span(k)
        got = urecv[k].astype(f32)
        is_upper = upper == 1
        upre[...] = upre[...] + jnp.where(is_upper, 0.0, decay_over(me + 1, high)) * got
        mine = jnp.where(is_upper, decay_over(low - (1 << k), low), 1.0)
        theirs = jnp.where(is_upper, 1.0, decay_over(low, high))
        utot[...] = mine * utot[...] + theirs * got

    strides = [n_sp >> (k + 1) for k in range(bits)]

    def mix_hop(k, base, c):
        block = lax.rem(base, 2 * strides[k]) + c * 2 * strides[k]
        block = lax.rem(block, n_sp)
        partner = me + strides[k] * (1 - 2 * lax.rem(me // strides[k], 2))
        ref = gmix.at[block]
        return remote(ref, ref, c_mix.send.at[k, c], c_mix.recv.at[block], (partner, tp))

    def widen(k):
        def one(c):
            mix_hop(k, me, c).start()

        loop(0, n_sp // (2 * strides[k]), one)

    def arrive(k):
        partner = me + strides[k] * (1 - 2 * lax.rem(me // strides[k], 2))

        def one(c):
            mix_hop(k, partner, c).wait_recv()
            mix_hop(k, me, c).wait_send()

        loop(0, n_sp // (2 * strides[k]), one)

    own_mix = pltpu.make_async_copy(mixed, gmix.at[me], own_sem)
    own_mix.start()
    own_mix.wait()
    widen(0)
    give(c_fwd, fsend, frecv, ftot, 0)
    sc_s[...] = jnp.where(causal, dot(qd_s[...], kg_s[...], NT, True), 0.0)
    for i in range(2, 6):
        fetch(i).wait()

    def half(j, p):
        block = near if j == 0 else near_far
        return remote(
            part.at[p, :, columns(block)], in1.at[p, j], c_half.send.at[j, p], c_half.recv.at[j, p], (me, near)
        )

    def cross(p):
        return remote(out1.at[p], in2.at[p], c_cross.send.at[p], c_cross.recv.at[p], (me, far))

    def back(p, slot):
        return remote(out2.at[p], ret.at[slot], c_back.send.at[p], c_back.recv.at[slot], (p, tp))

    def expert(m):
        p = flip(m)

        @pl.when(m > 0)
        def _():
            for j in (0, 1):
                beside(j, p, near).wait_recv()
                relay(j, p, near_far).wait_recv()

        x = gx[p].reshape(cap, width)
        dy = gdy[p].reshape(cap, width)
        gate = dot(x, wg[...], NN)
        up = dot(x, wu[...], NN)
        hidden_cot = dot(dy, wd[...], NT)
        sig = jax.nn.sigmoid(gate)
        hid[p] = (gate * sig * up).astype(bf16)
        gate_cot = (hidden_cot * up * sig * (1.0 + gate * (1.0 - sig))).astype(bf16)
        up_cot = (hidden_cot * gate * sig).astype(bf16)
        units = gate_cot.shape[1]
        cots[p, :, :units] = gate_cot
        cots[p, :, units:] = up_cot
        part[p] = (dot(gate_cot, wg[...], NT) + dot(up_cot, wu[...], NT)).astype(bf16)
        for j in (1, 0):
            half(j, p).start()

    def step(i):
        @pl.when((i >= 1) & (i < n_sp))
        def _():
            p = flip(i)
            for j in (0, 1):
                first(j, p, p).wait_recv()
                across(j, p, tp).start()
                beside(j, p, tp).start()

        @pl.when((i >= 2) & (i < n_sp + 2))
        def _():
            expert(i - 2)

        @pl.when((i >= 2) & (i < n_sp + 1))
        def _():
            p = flip(i - 1)
            for j in (0, 1):
                across(j, p, far).wait_recv()
                relay(j, p, far).start()

        @pl.when((i >= 3) & (i < n_sp + 3))
        def _():
            p = flip(i - 3)
            half(1, p).wait_recv()
            mine = part[p, :, columns(far)].astype(f32)
            out1[p] = (mine + in1[p, 1].astype(f32)).astype(bf16)
            cross(p).start()

        @pl.when(i >= 4)
        def _():
            p = flip(i - 4)
            half(0, p).wait_recv()
            cross(p).wait_recv()
            mine = part[p, :, columns(tp)].astype(f32)
            mine = mine + in1[p, 0].astype(f32)
            out2[p] = (mine + in2[p].astype(f32)).astype(bf16)

            @pl.when(i > 4)
            def _():
                back(p, me).start()

    loop(1, 4, step)

    def wait_decay(m):
        p = flip(m)
        decay(p, p).wait_recv()

    loop(1, n_sp, wait_decay)
    forward_merge(0)
    for k in range(1, bits):
        give(c_fwd, fsend, frecv, ftot, k)
        loop(2 + 2 * k, 4 + 2 * k, step)
        forward_merge(k)
    loop(2 + 2 * bits, n_sp + 4, step)
    ret[me] = out2[me]
    arrive(0)
    for k in range(1, bits):
        widen(k)
        if k < bits - 1:
            arrive(k)

    all_x = gx.reshape(n_sp * cap, width)
    all_dy = gdy.reshape(n_sp * cap, width)
    tile = 256

    def weight_grad(b):
        at = pl.ds(pl.multiple_of(b * tile, tile), tile)
        both = cots[...].reshape(n_sp * cap, cots.shape[2])
        units = cots.shape[2] // 2
        grads = dot(all_x[:, at], both, TN)
        grad_gate[at, :] = grads[:, :units]
        grad_up[at, :] = grads[:, units:]

    def down_grad(b):
        at = pl.ds(pl.multiple_of(b * tile, tile), tile)
        grad_down[:, at] = dot(hid[...].reshape(n_sp * cap, hid.shape[2]), all_dy[:, at], TN)

    loop(0, width // tile, weight_grad)

    def wait_back(m):
        p = flip(m)
        back(p, p).wait_recv()

    loop(1, n_sp, wait_back)
    acc = dot(comb[...], ret[...].reshape(n_sp * cap, quarter), NN)
    mid[:, columns(tp)] = (acc + dy_in[:, columns(tp)].astype(f32)).astype(bf16)

    def spread(k, block, device):
        ref = mid.at[:, columns(block)]
        return remote(ref, ref, c_share.send.at[k], c_share.recv.at[k], (me, device))

    def project(block):
        at = pl.ds(pl.multiple_of(block * quarter, quarter), quarter)
        return dot(mid[:, columns(block)], wo[at, :], NN)

    spread(0, tp, far).start()
    spread(1, tp, near).start()
    head[...] = project(tp)
    spread(1, near, near).wait_recv()
    head[...] += project(near)
    spread(0, far, far).wait_recv()
    spread(2, far, near).start()
    head[...] += project(far)
    spread(2, near_far, near).wait_recv()
    head[...] += project(near_far)

    utot[...] = dot(head[...], qd_s[...], TN, True)
    upre[...] = jnp.zeros_like(upre)
    give(c_rev, usend, urecv, utot, 0)

    def col_first(p, slot):
        at = pl.ds(pl.multiple_of(p * piece, piece), piece)
        mine = pl.ds(pl.multiple_of(tp * rows, rows), rows)
        return remote(
            mid.at[mine, at], gcols.at[slot, tp], d_first.send.at[p], d_first.recv.at[slot], (p, tp)
        )

    def col_pass(copies, p, block, device):
        ref = gcols.at[p, block]
        return remote(ref, ref, copies.send.at[p], copies.recv.at[p], (me, device))

    def send_cols(m):
        col_first(flip(m), me).start()

    loop(1, n_sp, send_cols)
    own_at = pl.ds(pl.multiple_of(me * piece, piece), piece)
    gcols[me] = mid[:, own_at].reshape(n_tp, rows, piece)
    scores_cot = jnp.where(causal, dot(head[...], vv[...].astype(f32), NT, True), 0.0)
    qc_s[...] = dot(scores_cot, kg_s[...], NN, True) + dot(head[...], fpre[...], NN, True)
    reverse_merge(0)
    give(c_rev, usend, urecv, utot, 1)
    kc_s[...] = dot(scores_cot, qd_s[...], TN, True)
    gv_s[...] = dot(sc_s[...], head[...], TN, True)
    for k in range(1, bits):
        reverse_merge(k)
        if k < bits - 1:
            give(c_rev, usend, urecv, utot, k + 1)

        if k == 1:
            def col_forward(m):
                p = flip(m)
                col_first(p, p).wait_recv()
                col_pass(d_across, p, tp, far).start()
                col_pass(d_beside, p, tp, near).start()

            loop(1, n_sp, col_forward)
            loop(0, width // tile, down_grad)

            def col_relay(m):
                p = flip(m)
                col_pass(d_across, p, far, far).wait_recv()
                col_pass(d_relay, p, far, near).start()

            loop(1, n_sp, col_relay)

    carry, enter = upre[...], fpre[...]
    cum = cum_s[...]
    total_decay = cum[tok - 1 : tok, :]
    val = vv[...].astype(f32)
    ke_cot = dot(val, carry, NN, True)
    grad_v[...] = (gv_s[...] + dot(ke_s[...], carry, NT, True)).astype(bf16)
    end = ke_cot * ke_s[...]
    c_cot = qc_s[...] * qd_s[...] - kc_s[...] * kg_s[...] - end
    last = jnp.sum(end, axis=0, keepdims=True) + jnp.exp(total_decay) * jnp.sum(
        carry * enter, axis=0, keepdims=True
    )
    grad_decay[...] = dot(lower, c_cot, TN, True) + last
    grad_q[...] = (qc_s[...] * jnp.exp(cum)).astype(bf16)
    grad_k[...] = (kc_s[...] * jnp.exp(-cum) + ke_cot * jnp.exp(total_decay - cum)).astype(bf16)

    arrive(bits - 1)

    def col_finish(m):
        p = flip(m)
        col_pass(d_beside, p, near, near).wait_recv()
        col_pass(d_relay, p, near_far, near).wait_recv()

    loop(1, n_sp, col_finish)
    grad_proj[...] = dot(
        gcols[...].reshape(n_sp * tok, piece), gmix[...].reshape(n_sp * tok, gmix.shape[2]), TN
    )

    def finish(m):
        p = flip(m)
        decay(p, me).wait_send()
        back(p, me).wait_send()
        col_first(p, me).wait_send()
        col_pass(d_across, p, tp, far).wait_send()
        col_pass(d_beside, p, tp, near).wait_send()
        col_pass(d_relay, p, far, near).wait_send()
        for j in (0, 1):
            first(j, p, me).wait_send()
            across(j, p, tp).wait_send()
            beside(j, p, tp).wait_send()
            relay(j, p, far).wait_send()

    loop(1, n_sp, finish)

    def finish_return(m):
        p = flip(m)
        cross(p).wait_send()
        for j in (0, 1):
            half(j, p).wait_send()

    loop(0, n_sp, finish_return)
    for k in range(bits):
        hop(c_fwd, fsend, frecv, k).wait_send()
        hop(c_rev, usend, urecv, k).wait_send()
    spread(0, tp, far).wait_send()
    spread(1, tp, near).wait_send()
    spread(2, far, near).wait_send()


def whole_plan(*args):
    bf16, f32 = jnp.bfloat16, jnp.float32
    n_sp, n_tp = lax.axis_size("sp"), lax.axis_size("tp")
    expert_in, route_ids, w_gate = args[0], args[2], args[4]
    tok, width = expert_in.shape
    units = w_gate.shape[2]
    cap = 2 * route_ids.shape[1] * tok // n_sp
    share, quarter, piece = cap // n_tp, width // n_tp, width // n_sp
    dv = args[11].shape[1]
    bits = n_sp.bit_length() - 1
    mem = pltpu.VMEM
    held = [
        mem(a.shape[1:] if a.ndim == 3 else a.shape, a.dtype) for a in args[:2] + args[4:]
    ]
    state = (dv, DK)
    scratch = held + [
        mem((128, tok), f32), mem((128, tok), f32), mem((tok, n_sp * cap), bf16),
        mem((n_sp, share, width), bf16), mem((n_sp, share, width), bf16),
        mem((n_sp, n_tp, share, width), bf16), mem((n_sp, n_tp, share, width), bf16),
        mem((n_sp, cap, 2 * units), bf16), mem((n_sp, cap, units), bf16), mem((n_sp, cap, width), bf16),
        mem((n_sp, 2, cap, quarter), bf16),
    ] + [mem((n_sp, cap, quarter), bf16)] * 4 + [
        mem((tok, width), bf16), mem((n_sp,) + args[8].shape, bf16), mem((n_sp, n_tp, tok // n_tp, piece), bf16),
        mem((n_sp, 8, DK), f32),
    ] + [mem((bits,) + state, bf16)] * 4 + [mem(state, f32)] * 4 + [mem((tok, dv), f32)] + [
        mem((tok, DK), f32)
    ] * 3 + [mem((tok, tok), f32), mem((tok, DK), f32), mem((tok, DK), f32), mem((tok, dv), f32), mem((tok, DK), f32)]
    scratch += [pltpu.SemaphoreType.DMA((11,)), pltpu.SemaphoreType.DMA]
    scratch += dma(2, n_sp) * 4 + dma(n_sp)
    scratch += [pltpu.SemaphoreType.DMA((bits, n_sp // 2)), pltpu.SemaphoreType.DMA((n_sp,))]
    scratch += dma(bits) + dma(2, n_sp) + dma(n_sp) * 2 + dma(3) + dma(bits) + dma(n_sp) * 4
    shapes = [
        ((width, units), f32), ((width, units), f32), ((units, width), f32), ((piece, args[8].shape[1]), f32),
        (args[9].shape, bf16), (args[10].shape, bf16), (args[11].shape, bf16), (args[12].shape, f32),
    ]
    outs = pl.pallas_call(
        functools.partial(whole_kernel, n_sp, n_tp),
        out_shape=tuple(jax.ShapeDtypeStruct(s, t) for s, t in shapes),
        in_specs=[ANY, ANY, VM, VM] + [ANY] * 9,
        out_specs=(VM,) * 8,
        scratch_shapes=scratch,
        compiler_params=pltpu.CompilerParams(
            collective_id=3, has_side_effects=True, vmem_limit_bytes=56 * 1024 * 1024
        ),
    )(*args)
    return tuple(a[None] for a in outs[:3]) + tuple(outs[3:])


def per_device(*args):
    n_sp, n_tp = lax.axis_size("sp"), lax.axis_size("tp")
    tok, top = args[0].shape[0], args[2].shape[1]
    heads = args[9].shape[1] // DK
    share = 2 * top * tok // (n_sp * n_tp)
    aligned = share % 16 == 0 and tok // n_tp % 16 == 0 and tok == 128
    if aligned and heads == 1 and args[4].shape[0] == 1 and n_tp == 4 and n_sp & (n_sp - 1) == 0:
        return whole_plan(*args)
    return spread_plan(*args)


def solution(mesh):
    tokens, both = P("sp", None), P("sp", "tp")
    up, down = P("sp", None, "tp"), P("sp", "tp", None)
    return jax.shard_map(
        per_device,
        mesh=mesh,
        in_specs=(tokens,) * 4 + (up, up, down, P(None, "tp")) + (both,) * 5,
        out_specs=(up, up, down) + (both,) * 5,
        check_vma=False,
    )
```

```python
import functools

import jax
import jax.numpy as jnp
from jax import lax
from jax.experimental import pallas as pl
from jax.experimental.pallas import tpu as pltpu
from jax.sharding import PartitionSpec as P

DK = 128
EXACT = lax.Precision.HIGHEST
MESH = pl.DeviceIdType.MESH


def remote(src, dst, send, recv, device):
    return pltpu.make_async_remote_copy(
        src_ref=src, dst_ref=dst, send_sem=send, recv_sem=recv, device_id=device, device_id_type=MESH
    )


def greet(n_sp, me, tp, partners):
    barrier = pltpu.get_barrier_semaphore()

    def hello(i, carry):
        pl.semaphore_signal(
            barrier, inc=1, device_id=(lax.rem(me + i, n_sp), tp), device_id_type=MESH
        )
        return carry

    lax.fori_loop(1, n_sp, hello, 0)
    for other in partners:
        pl.semaphore_signal(barrier, inc=1, device_id=(me, other), device_id_type=MESH)
    pl.semaphore_wait(barrier, n_sp - 1 + len(partners))


def loop(start, stop, body):
    def step(i, carry):
        body(i)
        return carry

    lax.fori_loop(start, stop, step, 0)


def spread_kernel(n_sp, n_tp, n_rows, n_sides, *refs):
    count = n_rows + n_sides
    given, got = refs[:count], refs[count : 2 * count]
    s0, r0, s1, r1, s2, r2, s3, r3, s4, r4, own_sem = refs[2 * count :]
    me, tp = lax.axis_index("sp"), lax.axis_index("tp")
    far = lax.rem(tp + n_tp // 2, n_tp)
    near = tp + 1 - 2 * lax.rem(tp, 2)
    greet(n_sp, me, tp, (far, near))
    rows = tuple(zip(given[:n_rows], got[:n_rows]))
    sides = tuple(zip(given[n_rows:], got[n_rows:]))

    def first(j, p, slot):
        return remote(rows[j][0].at[p], rows[j][1].at[slot, tp], s0.at[j, p], r0.at[j, slot], (p, tp))

    def across(j, p, share):
        ref = rows[j][1].at[p, share]
        return remote(ref, ref, s1.at[j, p], r1.at[j, p], (me, far))

    def beside(j, p, share):
        ref = rows[j][1].at[p, share]
        return remote(ref, ref, s2.at[j, p], r2.at[j, p], (me, near))

    def relay(j, p, share):
        ref = rows[j][1].at[p, share]
        return remote(ref, ref, s3.at[j, p], r3.at[j, p], (me, near))

    def side(k, p, slot):
        return remote(sides[k][0], sides[k][1].at[slot], s4.at[k, p], r4.at[k, slot], (p, tp))

    def send(i):
        p = lax.rem(me + i, n_sp)
        for j in range(n_rows):
            first(j, p, me).start()

    loop(1, n_sp, send)
    owns = [
        pltpu.make_async_copy(rows[j][0].at[me], rows[j][1].at[me, tp], own_sem.at[j]) for j in range(n_rows)
    ] + [pltpu.make_async_copy(sides[k][0], sides[k][1].at[me], own_sem.at[n_rows + k]) for k in range(n_sides)]
    for own in owns:
        own.start()
    for own in owns:
        own.wait()
    for j in range(n_rows):
        across(j, me, tp).start()
        beside(j, me, tp).start()

    def send_side(i):
        p = lax.rem(me + i, n_sp)
        for k in range(n_sides):
            side(k, p, me).start()

    loop(1, n_sp, send_side)

    def forward(i):
        p = lax.rem(me - i + n_sp, n_sp)
        for j in range(n_rows):
            first(j, p, p).wait_recv()
            across(j, p, tp).start()
            beside(j, p, tp).start()

    loop(1, n_sp, forward)

    def pass_on(i):
        p = lax.rem(me - i + n_sp, n_sp)
        for j in range(n_rows):
            across(j, p, far).wait_recv()
            relay(j, p, far).start()

    loop(0, n_sp, pass_on)
    near_far = lax.rem(near + n_tp // 2, n_tp)

    def finish(i):
        p = lax.rem(me - i + n_sp, n_sp)
        for j in range(n_rows):
            beside(j, p, near).wait_recv()
            relay(j, p, near_far).wait_recv()
            across(j, p, tp).wait_send()
            beside(j, p, tp).wait_send()
            relay(j, p, far).wait_send()

    loop(0, n_sp, finish)

    def finish_side(i):
        p = lax.rem(me - i + n_sp, n_sp)
        for k in range(n_sides):
            side(k, p, p).wait_recv()
            side(k, p, me).wait_send()
        for j in range(n_rows):
            first(j, p, me).wait_send()

    loop(1, n_sp, finish_side)


def return_kernel(
    n_sp, n_tp, part, comb, dy, mix, state, mid, gmix, gstate, in1, out1, in2, out2, ret,
    s1, r1, s2, r2, s3, r3, s4, r4, s5, r5, own_sem,
):
    me, tp = lax.axis_index("sp"), lax.axis_index("tp")
    far = lax.rem(tp + n_tp // 2, n_tp)
    near = tp + 1 - 2 * lax.rem(tp, 2)
    near_far = lax.rem(near + n_tp // 2, n_tp)
    quarter = part.shape[2] // n_tp
    greet(n_sp, me, tp, (far, near))

    gathered = ((mix, gmix), (state, gstate))
    strides = [n_sp >> (k + 1) for k in range(n_sp.bit_length() - 1)]

    def hop(j, k, base, c):
        block = lax.rem(base, 2 * strides[k]) + c * 2 * strides[k]
        partner = me + strides[k] * (1 - 2 * lax.rem(me // strides[k], 2))
        ref = gathered[j][1].at[block]
        return remote(ref, ref, s5.at[j, k, c], r5.at[j, block], (partner, tp))

    def widen(k):
        def one(c):
            for j in (0, 1):
                hop(j, k, me, c).start()

        loop(0, n_sp // (2 * strides[k]), one)

    def arrive(k):
        partner = me + strides[k] * (1 - 2 * lax.rem(me // strides[k], 2))

        def one(c):
            for j in (0, 1):
                hop(j, k, partner, c).wait_recv()
                hop(j, k, me, c).wait_send()

        loop(0, n_sp // (2 * strides[k]), one)

    def columns(block):
        return pl.ds(pl.multiple_of(block * quarter, quarter), quarter)

    def beside(j, p):
        block = near if j == 0 else near_far
        return remote(
            part.at[p, :, columns(block)], in1.at[p, j], s1.at[j, p], r1.at[j, p], (me, near)
        )

    def across(p):
        return remote(out1.at[p], in2.at[p], s2.at[p], r2.at[p], (me, far))

    def back(p, slot):
        return remote(out2.at[p], ret.at[slot], s3.at[p], r3.at[slot], (p, tp))

    def start(i):
        p = lax.rem(me + 1 + i, n_sp)
        for j in (1, 0):
            beside(j, p).start()

    loop(0, n_sp, start)
    owns = [
        pltpu.make_async_copy(gathered[j][0], gathered[j][1].at[me], own_sem.at[j]) for j in (0, 1)
    ]
    for own in owns:
        own.start()
    for own in owns:
        own.wait()
    widen(0)

    def pair(i):
        p = lax.rem(me + 1 + i, n_sp)
        beside(1, p).wait_recv()
        mine = part[p, :, columns(far)].astype(jnp.float32)
        out1[p] = (mine + in1[p, 1].astype(jnp.float32)).astype(jnp.bfloat16)
        across(p).start()

    loop(0, n_sp, pair)
    arrive(0)
    for k in range(1, len(strides) - 1):
        widen(k)
        arrive(k)

    def total(p):
        beside(0, p).wait_recv()
        across(p).wait_recv()
        mine = part[p, :, columns(tp)].astype(jnp.float32)
        mine = mine + in1[p, 0].astype(jnp.float32)
        return (mine + in2[p].astype(jnp.float32)).astype(jnp.bfloat16)

    def quad(i):
        p = lax.rem(me + i, n_sp)
        out2[p] = total(p)
        back(p, me).start()

    loop(1, n_sp, quad)
    ret[me] = total(me)
    widen(len(strides) - 1)

    def gather(i, acc):
        p = lax.rem(me - i + n_sp, n_sp)

        @pl.when(i > 0)
        def _():
            back(p, p).wait_recv()

        return acc + jnp.dot(comb[p], ret[p], preferred_element_type=jnp.float32)

    acc = lax.fori_loop(0, n_sp, gather, dy[:, columns(tp)].astype(jnp.float32))
    mid[:, columns(tp)] = acc.astype(jnp.bfloat16)

    def share(k, block, device):
        ref = mid.at[:, columns(block)]
        return remote(ref, ref, s4.at[k], r4.at[k], (me, device))

    share(0, tp, far).start()
    share(1, tp, near).start()
    share(0, far, far).wait_recv()
    share(2, far, near).start()
    share(1, near, near).wait_recv()
    share(2, near_far, near).wait_recv()
    share(0, tp, far).wait_send()
    share(1, tp, near).wait_send()
    share(2, far, near).wait_send()

    arrive(len(strides) - 1)

    def finish(i):
        p = lax.rem(me + i, n_sp)
        for j in (0, 1):
            beside(j, p).wait_send()
        across(p).wait_send()

        @pl.when(i > 0)
        def _():
            back(p, me).wait_send()

    loop(0, n_sp, finish)


VM = pl.BlockSpec(memory_space=pltpu.VMEM)
ANY = pl.BlockSpec(memory_space=pl.ANY)


def dma(*shape):
    return [pltpu.SemaphoreType.DMA(shape), pltpu.SemaphoreType.DMA(shape)]


def call(kernel, ident, operands, in_specs, out_shape, out_specs, scratch):
    return pl.pallas_call(
        kernel,
        out_shape=out_shape,
        in_specs=in_specs,
        out_specs=out_specs,
        scratch_shapes=scratch,
        compiler_params=pltpu.CompilerParams(
            collective_id=ident, has_side_effects=True, vmem_limit_bytes=48 * 1024 * 1024
        ),
    )(*operands)


def spread_plan(
    expert_in, out_cot, route_ids, route_weights, w_gate, w_up, w_down, w_out,
    mixed_heads, queries, keys, values, log_decay,
):
    bf16, f32 = jnp.bfloat16, jnp.float32
    n_sp, n_tp = lax.axis_size("sp"), lax.axis_size("tp")
    me, tp = lax.axis_index("sp"), lax.axis_index("tp")
    tok, width = expert_in.shape
    top = route_ids.shape[1]
    experts = w_gate.shape[0] * n_sp
    cap = 2 * top * tok // experts
    share = cap // n_tp

    ids = route_ids.reshape(-1)
    onehot = ids[:, None] == jnp.arange(experts, dtype=jnp.int32)
    order = jnp.arange(tok * top, dtype=jnp.int32)
    below = (order[None, :] < order[:, None]).astype(bf16)
    ranks = jnp.dot(below, onehot.astype(bf16), preferred_element_type=f32)
    rank = jnp.sum(jnp.where(onehot, ranks, 0.0), axis=1).astype(jnp.int32)
    slot = (ids * cap + rank).reshape(tok, top)
    mine = (
        jnp.arange(experts, dtype=jnp.int32)[:, None] * cap
        + tp * share
        + jnp.arange(share, dtype=jnp.int32)[None, :]
    ).reshape(-1)
    match = slot[None] == mine[:, None, None]
    pick = jnp.any(match, axis=2).astype(bf16)
    slot_weight = jnp.sum(jnp.where(match, route_weights[None], 0.0), axis=(1, 2))
    x_share = jnp.dot(pick, expert_in, preferred_element_type=f32).astype(bf16)
    dy_share = (
        slot_weight[:, None] * jnp.dot(pick, out_cot, preferred_element_type=f32)
    ).astype(bf16)
    places = jnp.arange(experts * cap, dtype=jnp.int32).reshape(experts, 1, cap, 1)
    comb = jnp.any(slot[None, :, None, :] == places, axis=3).astype(bf16)

    heads = queries.shape[1] // DK
    dv = values.shape[1] // heads
    step = jnp.arange(tok, dtype=jnp.int32)
    causal = step[None, :] <= step[:, None]
    lower = causal.astype(f32)
    cumulative = jnp.dot(lower, log_decay, precision=EXACT)
    decay_sum = cumulative[-1:]

    def split(array):
        return array.astype(f32).reshape(tok, heads, -1)

    q, k, v = split(queries), split(keys), split(values)
    grow, shrink, to_end = (
        split(jnp.exp(-cumulative)),
        split(jnp.exp(cumulative)),
        split(jnp.exp(decay_sum - cumulative)),
    )
    qd, kg, ke = q * shrink, k * grow, k * to_end
    state_local = jnp.einsum("thd,the->hde", ke, v, precision=EXACT)

    rows = jax.ShapeDtypeStruct((n_sp, n_tp, share, width), bf16)
    gx, gdy, gdecay = call(
        functools.partial(spread_kernel, n_sp, n_tp, 2, 1),
        0,
        (
            x_share.reshape(n_sp, share, width),
            dy_share.reshape(n_sp, share, width),
            decay_sum,
        ),
        [VM] * 3,
        (
            rows,
            rows,
            jax.ShapeDtypeStruct((n_sp,) + decay_sum.shape, f32),
        ),
        (ANY, ANY, ANY),
        dma(2, n_sp) * 4 + dma(1, n_sp) + [pltpu.SemaphoreType.DMA((3,))],
    )
    got_x = gx.reshape(n_sp * cap, width)
    got_dy = gdy.reshape(n_sp * cap, width)
    wg, wu, wd = w_gate[0], w_up[0], w_down[0]
    gate_pre = jnp.dot(got_x, wg, preferred_element_type=f32)
    up_pre = jnp.dot(got_x, wu, preferred_element_type=f32)
    hidden_cot = lax.dot_general(got_dy, wd, (((1,), (1,)), ((), ())), preferred_element_type=f32)
    sig = jax.nn.sigmoid(gate_pre)
    hidden = (gate_pre * sig * up_pre).astype(bf16)
    gate_cot = (hidden_cot * up_pre * sig * (1.0 + gate_pre * (1.0 - sig))).astype(bf16)
    up_cot = (hidden_cot * gate_pre * sig).astype(bf16)
    back = (((1,), (1,)), ((), ()))
    part = lax.dot_general(gate_cot, wg, back, preferred_element_type=f32) + lax.dot_general(
        up_cot, wu, back, preferred_element_type=f32
    )
    part = part.astype(bf16).reshape(n_sp, cap, width)
    over = (((0,), (0,)), ((), ()))
    grad_gate = lax.dot_general(got_x, gate_cot, over, preferred_element_type=f32)[None]
    grad_up = lax.dot_general(got_x, up_cot, over, preferred_element_type=f32)[None]
    grad_down = lax.dot_general(hidden, got_dy, over, preferred_element_type=f32)[None]

    quarter = width // n_tp
    buf = pltpu.VMEM((n_sp, cap, quarter), bf16)
    mid, gmix, gstate = call(
        functools.partial(return_kernel, n_sp, n_tp),
        1,
        (part, comb, out_cot, mixed_heads, state_local.reshape(heads * DK, dv).astype(bf16)),
        [VM] * 5,
        (
            jax.ShapeDtypeStruct((tok, width), bf16),
            jax.ShapeDtypeStruct((n_sp,) + mixed_heads.shape, bf16),
            jax.ShapeDtypeStruct((n_sp, heads * DK, dv), bf16),
        ),
        (VM, VM, VM),
        [pltpu.VMEM((n_sp, 2, cap, quarter), bf16), buf, buf, buf, buf]
        + dma(2, n_sp) + dma(n_sp) + dma(n_sp) + dma(3)
        + [
            pltpu.SemaphoreType.DMA((2, n_sp.bit_length() - 1, n_sp // 2)),
            pltpu.SemaphoreType.DMA((2, n_sp)),
            pltpu.SemaphoreType.DMA((2,)),
        ],
    )
    head_cot = split(jnp.dot(mid, w_out, preferred_element_type=f32))
    pull = jnp.einsum("thd,the->hde", qd, head_cot, precision=EXACT)
    part_tok = tok // n_tp
    cols = lax.dynamic_slice_in_dim(mid, tp * part_tok, part_tok, 0)
    cols = cols.reshape(part_tok, n_sp, width // n_sp).swapaxes(0, 1)
    gcols, gpull = call(
        functools.partial(spread_kernel, n_sp, n_tp, 1, 1),
        2,
        (cols, pull.reshape(heads * DK, dv).astype(bf16)),
        [VM] * 2,
        (
            jax.ShapeDtypeStruct((n_sp, n_tp, part_tok, width // n_sp), bf16),
            jax.ShapeDtypeStruct((n_sp, heads * DK, dv), bf16),
        ),
        (VM, VM),
        dma(1, n_sp) * 5 + [pltpu.SemaphoreType.DMA((2,))],
    )
    gcols = gcols.reshape(n_sp, tok, width // n_sp)
    grad_out_proj = jnp.einsum("ntd,nte->de", gcols, gmix, preferred_element_type=f32)

    sums = gdecay[:, 0]
    index = jnp.arange(n_sp, dtype=jnp.int32)
    between = (index[None] > jnp.minimum(index, me)[:, None]) & (
        index[None] < jnp.maximum(index, me)[:, None]
    )
    weight = jnp.exp(jnp.sum(jnp.where(between[..., None], sums[None], 0.0), axis=1))

    def entering(pieces, used):
        scale = jnp.where(used[:, None], weight, 0.0)
        return jnp.sum(scale[..., None] * pieces.astype(f32), axis=0).reshape(heads, DK, dv)

    state_in = entering(gstate, index < me)
    state_cot = entering(gpull, index > me)

    dot = functools.partial(jnp.einsum, precision=EXACT)
    scores = jnp.where(causal, dot("thd,shd->hts", qd, kg), 0.0)
    scores_cot = jnp.where(causal, dot("the,she->hts", head_cot, v), 0.0)
    grad_v = dot("hts,the->she", scores, head_cot) + dot("shd,hde->she", ke, state_cot)
    qd_cot = dot("hts,shd->thd", scores_cot, kg) + dot("the,hde->thd", head_cot, state_in)
    kg_cot = dot("hts,thd->shd", scores_cot, qd)
    ke_cot = dot("she,hde->shd", v, state_cot)
    end = ke_cot * ke
    c_cot = (qd_cot * qd - kg_cot * kg - end).reshape(tok, heads * DK)
    last = jnp.sum(end, axis=0).reshape(-1) + jnp.exp(decay_sum[0]) * jnp.sum(
        state_cot * state_in, axis=2
    ).reshape(-1)
    grad_decay = lax.dot_general(lower, c_cot, over, precision=EXACT) + last[None]
    grad_q = (qd_cot * shrink).astype(bf16).reshape(tok, heads * DK)
    grad_k = (kg_cot * grow + ke_cot * to_end).astype(bf16).reshape(tok, heads * DK)
    return (
        grad_gate,
        grad_up,
        grad_down,
        grad_out_proj,
        grad_q,
        grad_k,
        grad_v.astype(bf16).reshape(tok, heads * dv),
        grad_decay,
    )


class Copies:
    def __init__(self, send, recv):
        self.send, self.recv = send, recv


def dot(a, b, dims, exact=False):
    return lax.dot_general(
        a, b, (dims, ((), ())), precision=EXACT if exact else None, preferred_element_type=jnp.float32
    )


NN, NT, TN = ((1,), (0,)), ((1,), (1,)), ((0,), (0,))


def whole_kernel(n_sp, n_tp, *refs):
    bf16, f32 = jnp.bfloat16, jnp.float32
    given, refs = refs[:13], refs[13:]
    outs, refs = refs[:8], refs[8:]
    x_hbm, dy_hbm, ids, weights, *_ = given
    grad_gate, grad_up, grad_down, grad_proj, grad_q, grad_k, grad_v, grad_decay = outs
    (
        x_in, dy_in, wg, wu, wd, wo, mixed, qv, kv, vv, gv,
        pos_t, wt, comb, xs, dys, gx, gdy, cots, hid, part, in1, out1, in2, out2, ret,
        mid, gmix, gcols, dall, fsend, frecv, usend, urecv, ftot, fpre, utot, upre,
        head, qd_s, kg_s, ke_s, sc_s, qc_s, kc_s, gv_s, cum_s,
        load, own_sem, *sems,
    ) = refs
    pairs = [Copies(a, b) for a, b in zip(sems[::2], sems[1::2])]
    (
        c_first, c_across, c_beside, c_relay, c_sum, c_mix, c_fwd, c_half, c_cross, c_back,
        c_share, c_rev, c_second, d_first, d_across, d_beside, d_relay,
    ) = pairs
    me, tp = lax.axis_index("sp"), lax.axis_index("tp")
    far = lax.rem(tp + n_tp // 2, n_tp)
    near = tp + 1 - 2 * lax.rem(tp, 2)
    near_far = lax.rem(near + n_tp // 2, n_tp)
    tok, width = x_in.shape
    share = xs.shape[2]
    cap = share * n_tp
    quarter = width // n_tp
    piece = width // n_sp
    rows = tok // n_tp
    bits = n_sp.bit_length() - 1
    close = 2

    sources = (x_hbm, dy_hbm) + tuple(given[4:])
    places = (x_in, dy_in, wg, wu, wd, wo, mixed, qv, kv, vv, gv)

    def fetch(i):
        src = sources[i].at[0] if len(sources[i].shape) == 3 else sources[i]
        return pltpu.make_async_copy(src, places[i], load.at[i])

    for i in range(len(places)):
        fetch(i).start()

    barrier = pltpu.get_barrier_semaphore()

    def hello(i):
        pl.semaphore_signal(
            barrier, inc=1, device_id=(lax.rem(me + i, n_sp), tp), device_id_type=MESH
        )

    loop(1, n_sp, hello)
    for other in (far, near):
        pl.semaphore_signal(barrier, inc=1, device_id=(me, other), device_id_type=MESH)

    def flip(m):
        out = 0
        for b in range(bits):
            a, c = lax.rem(me // (1 << b), 2), lax.rem(m // (1 << b), 2)
            out = out + (1 << b) * (a + c - 2 * a * c)
        return out

    def turn(i):
        zero = 1 - (i + n_sp - 1) // n_sp
        is_near = lax.rem(i, 2) * (1 - i // (n_sp - 1)) + zero
        half_way = (i + 1) // 2
        return half_way + (1 - is_near) * (n_sp // 2 - 1)

    def peer(i):
        return flip(turn(i))

    def columns(block):
        return pl.ds(pl.multiple_of(block * quarter, quarter), quarter)

    down = lax.broadcasted_iota(jnp.int32, (tok, tok), 0)
    across_i = lax.broadcasted_iota(jnp.int32, (tok, tok), 1)
    weight, hit = jnp.zeros((tok, tok), f32), jnp.zeros((tok, tok), f32)
    for j in range(ids.shape[0]):
        hit_j = ids[j : j + 1, :] == down
        weight = weight + jnp.where(hit_j, weights[j : j + 1, :], 0.0)
        hit = hit + jnp.where(hit_j, 1.0, 0.0)
    above = jnp.where(down < across_i, 1.0, 0.0).astype(bf16)
    pos = jnp.where(hit > 0.5, dot(hit.astype(bf16), above, NN), -1.0)
    pos_t[...] = pos
    wt[...] = weight
    pos = jnp.transpose(pos)
    slot_lane = lax.broadcasted_iota(jnp.int32, (tok, cap), 1).astype(f32)
    for e in range(n_sp):
        comb[:, e * cap : (e + 1) * cap] = jnp.where(pos[:, e : e + 1] == slot_lane, 1.0, 0.0).astype(bf16)

    fetch(0).wait()
    fetch(1).wait()

    def chosen(e, start, count):
        want = (lax.broadcasted_iota(jnp.int32, (count, tok), 0) + start).astype(f32)
        match = pos_t[pl.ds(e, 1), :] == want
        scale = jnp.sum(jnp.where(match, wt[pl.ds(e, 1), :], 0.0), axis=1, keepdims=True)
        return jnp.where(match, 1.0, 0.0), scale

    found = [chosen(e, block * share, share) for e in range(n_sp) for block in (tp, far)]
    pick = jnp.concatenate([a for a, _ in found], axis=0).astype(bf16)
    scale = jnp.concatenate([b for _, b in found], axis=0)
    xs[...] = dot(pick, x_in[...], NN).astype(bf16).reshape(n_sp, 2, share, width)
    dys[...] = (scale * dot(pick, dy_in[...], NN)).astype(bf16).reshape(n_sp, 2, share, width)

    pl.semaphore_wait(barrier, n_sp + 1)

    row_pairs = ((xs, gx), (dys, gdy))

    def first(j, p, slot):
        return remote(
            row_pairs[j][0].at[p, 0], row_pairs[j][1].at[slot, tp],
            c_first.send.at[j, p], c_first.recv.at[j, slot], (p, tp),
        )

    def second(j, p, slot):
        return remote(
            row_pairs[j][0].at[p, 1], row_pairs[j][1].at[slot, far],
            c_second.send.at[j, p], c_second.recv.at[j, slot], (p, tp),
        )

    def passing(copies, j, p, block, device):
        ref = row_pairs[j][1].at[p, block]
        return remote(ref, ref, copies.send.at[j, p], copies.recv.at[j, p], (me, device))

    def across(j, p, block):
        return passing(c_across, j, p, block, far)

    def beside(j, p, block):
        return passing(c_beside, j, p, block, near)

    def relay(j, p, block):
        return passing(c_relay, j, p, block, near)

    def dispatch(m):
        p = peer(m)
        for j in (0, 1):
            first(j, p, me).start()

            @pl.when(m < close)
            def _():
                second(j, p, me).start()

    loop(1, n_sp, dispatch)

    own_pick, own_scale = chosen(me, 0, cap)
    own_pick = own_pick.astype(bf16)
    gx[me] = dot(own_pick, x_in[...], NN).astype(bf16).reshape(n_tp, share, width)
    gdy[me] = (own_scale * dot(own_pick, dy_in[...], NN)).astype(bf16).reshape(n_tp, share, width)

    for i in range(6, 11):
        fetch(i).wait()
    causal = across_i <= down
    lower = jnp.where(causal, 1.0, 0.0)
    cum = dot(lower, gv[...], NN, True)
    total_decay = cum[tok - 1 : tok, :]
    cum_s[...] = cum
    dall[me] = jnp.broadcast_to(total_decay, dall.shape[1:])

    def decay(p, slot):
        return remote(dall.at[me], dall.at[slot], c_sum.send.at[p], c_sum.recv.at[slot], (p, tp))

    def send_decay(m):
        decay(flip(m), me).start()

    loop(1, n_sp, send_decay)
    key = kv[...].astype(f32)
    val = vv[...].astype(f32)
    qd_s[...] = qv[...].astype(f32) * jnp.exp(cum)
    kg_s[...] = key * jnp.exp(-cum)
    ke_s[...] = key * jnp.exp(total_decay - cum)
    ftot[...] = dot(val, ke_s[...], TN, True)
    fpre[...] = jnp.zeros_like(fpre)

    def hop(copies, held, got, k):
        partner = me + (1 << k) * (1 - 2 * lax.rem(me // (1 << k), 2))
        return remote(held.at[k], got.at[k], copies.send.at[k], copies.recv.at[k], (partner, tp))

    def give(copies, held, got, total, k):
        held[k] = total[...].astype(bf16)
        hop(copies, held, got, k).start()

    def decay_over(low, high):
        table = dall[:, 0, :]
        index = lax.broadcasted_iota(jnp.int32, table.shape, 0)
        picked = jnp.where((index >= low) & (index < high), table, 0.0)
        return jnp.exp(jnp.sum(picked, axis=0, keepdims=True))

    def span(k):
        size = 1 << k
        base = me - lax.rem(me, size)
        upper = lax.rem(me // size, 2)
        return base, base + size, upper

    def forward_merge(k):
        hop(c_fwd, fsend, frecv, k).wait_recv()
        low, high, upper = span(k)
        got = frecv[k].astype(f32)
        is_upper = upper == 1
        fpre[...] = fpre[...] + jnp.where(is_upper, decay_over(low, me), 0.0) * got
        mine = jnp.where(is_upper, 1.0, decay_over(low + (1 << k), high + (1 << k)))
        theirs = jnp.where(is_upper, decay_over(low, high), 1.0)
        ftot[...] = mine * ftot[...] + theirs * got

    def reverse_merge(k):
        hop(c_rev, usend, urecv, k).wait_recv()
        low, high, upper = span(k)
        got = urecv[k].astype(f32)
        is_upper = upper == 1
        upre[...] = upre[...] + jnp.where(is_upper, 0.0, decay_over(me + 1, high)) * got
        mine = jnp.where(is_upper, decay_over(low - (1 << k), low), 1.0)
        theirs = jnp.where(is_upper, 1.0, decay_over(low, high))
        utot[...] = mine * utot[...] + theirs * got

    strides = [n_sp >> (k + 1) for k in range(bits)]

    def mix_hop(k, base, c):
        block = lax.rem(base, 2 * strides[k]) + c * 2 * strides[k]
        block = lax.rem(block, n_sp)
        partner = me + strides[k] * (1 - 2 * lax.rem(me // strides[k], 2))
        ref = gmix.at[block]
        return remote(ref, ref, c_mix.send.at[k, c], c_mix.recv.at[block], (partner, tp))

    def widen(k):
        def one(c):
            mix_hop(k, me, c).start()

        loop(0, n_sp // (2 * strides[k]), one)

    def arrive(k):
        partner = me + strides[k] * (1 - 2 * lax.rem(me // strides[k], 2))

        def one(c):
            mix_hop(k, partner, c).wait_recv()
            mix_hop(k, me, c).wait_send()

        loop(0, n_sp // (2 * strides[k]), one)

    own_mix = pltpu.make_async_copy(mixed, gmix.at[me], own_sem)
    own_mix.start()
    own_mix.wait()
    widen(0)
    give(c_fwd, fsend, frecv, ftot, 0)
    sc_s[...] = jnp.where(causal, dot(qd_s[...], kg_s[...], NT, True), 0.0)
    for i in range(2, 6):
        fetch(i).wait()

    def half(j, p):
        block = near if j == 0 else near_far
        return remote(
            part.at[p, :, columns(block)], in1.at[p, j], c_half.send.at[j, p], c_half.recv.at[j, p], (me, near)
        )

    def cross(p):
        return remote(out1.at[p], in2.at[p], c_cross.send.at[p], c_cross.recv.at[p], (me, far))

    def back(p, slot):
        return remote(out2.at[p], ret.at[slot], c_back.send.at[p], c_back.recv.at[slot], (p, tp))

    def expert(m):
        p = peer(m)

        @pl.when(m > 0)
        def _():
            for j in (0, 1):
                beside(j, p, near).wait_recv()
                relay(j, p, near_far).wait_recv()

        x = gx[p].reshape(cap, width)
        dy = gdy[p].reshape(cap, width)
        gate = dot(x, wg[...], NN)
        up = dot(x, wu[...], NN)
        hidden_cot = dot(dy, wd[...], NT)
        sig = jax.nn.sigmoid(gate)
        hid[p] = (gate * sig * up).astype(bf16)
        gate_cot = (hidden_cot * up * sig * (1.0 + gate * (1.0 - sig))).astype(bf16)
        up_cot = (hidden_cot * gate * sig).astype(bf16)
        units = gate_cot.shape[1]
        cots[p, :, :units] = gate_cot
        cots[p, :, units:] = up_cot
        part[p] = (dot(gate_cot, wg[...], NT) + dot(up_cot, wu[...], NT)).astype(bf16)
        for j in (1, 0):
            half(j, p).start()

    def step(i):
        @pl.when((i >= 3) & (i < n_sp + 3))
        def _():
            p = peer(i - 3)
            half(1, p).wait_recv()
            mine = part[p, :, columns(far)].astype(f32)
            out1[p] = (mine + in1[p, 1].astype(f32)).astype(bf16)
            cross(p).start()

        @pl.when(i < n_sp)
        def _():
            p = peer(i)
            for j in (0, 1):
                first(j, p, p).wait_recv()

                @pl.when(i >= close)
                def _():
                    across(j, p, tp).start()

                beside(j, p, tp).start()

        @pl.when((i >= 3) & (i < n_sp + 2))
        def _():
            expert(i - 2)

        @pl.when((i >= 2) & (i < n_sp + 1))
        def _():
            p = peer(i - 1)
            for j in (0, 1):

                @pl.when(i - 1 >= close)
                def _():
                    across(j, p, far).wait_recv()

                @pl.when(i - 1 < close)
                def _():
                    second(j, p, p).wait_recv()

                relay(j, p, far).start()

        @pl.when(i >= 4)
        def _():
            p = peer(i - 4)
            half(0, p).wait_recv()
            cross(p).wait_recv()
            mine = part[p, :, columns(tp)].astype(f32)
            mine = mine + in1[p, 0].astype(f32)
            out2[p] = (mine + in2[p].astype(f32)).astype(bf16)

            @pl.when(i > 4)
            def _():
                back(p, me).start()

    expert(0)
    loop(1, n_sp + 4, step)
    ret[me] = out2[me]

    def wait_decay(m):
        p = flip(m)
        decay(p, p).wait_recv()

    all_x = gx.reshape(n_sp * cap, width)
    all_dy = gdy.reshape(n_sp * cap, width)
    tile = 256

    def weight_grad(b):
        at = pl.ds(pl.multiple_of(b * tile, tile), tile)
        both = cots[...].reshape(n_sp * cap, cots.shape[2])
        units = cots.shape[2] // 2
        grads = dot(all_x[:, at], both, TN)
        grad_gate[at, :] = grads[:, :units]
        grad_up[at, :] = grads[:, units:]

    def down_grad(b):
        at = pl.ds(pl.multiple_of(b * tile, tile), tile)
        grad_down[:, at] = dot(hid[...].reshape(n_sp * cap, hid.shape[2]), all_dy[:, at], TN)

    loop(0, width // tile, weight_grad)

    def wait_back(m):
        p = flip(m)
        back(p, p).wait_recv()

    loop(1, n_sp, wait_back)
    acc = dot(comb[...], ret[...].reshape(n_sp * cap, quarter), NN)
    mid[:, columns(tp)] = (acc + dy_in[:, columns(tp)].astype(f32)).astype(bf16)

    def spread(k, block, device):
        ref = mid.at[:, columns(block)]
        return remote(ref, ref, c_share.send.at[k], c_share.recv.at[k], (me, device))

    def project(block):
        at = pl.ds(pl.multiple_of(block * quarter, quarter), quarter)
        return dot(mid[:, columns(block)], wo[at, :], NN)

    spread(0, tp, far).start()
    spread(1, tp, near).start()
    loop(1, n_sp, wait_decay)
    forward_merge(0)
    give(c_fwd, fsend, frecv, ftot, 1)
    arrive(0)
    widen(1)
    head[...] = project(tp)
    spread(1, near, near).wait_recv()
    head[...] += project(near)
    spread(0, far, far).wait_recv()
    spread(2, far, near).start()
    head[...] += project(far)
    spread(2, near_far, near).wait_recv()
    head[...] += project(near_far)

    utot[...] = dot(head[...], qd_s[...], TN, True)
    upre[...] = jnp.zeros_like(upre)
    give(c_rev, usend, urecv, utot, 0)

    def col_first(p, slot):
        at = pl.ds(pl.multiple_of(p * piece, piece), piece)
        mine = pl.ds(pl.multiple_of(tp * rows, rows), rows)
        return remote(
            mid.at[mine, at], gcols.at[slot, tp], d_first.send.at[p], d_first.recv.at[slot], (p, tp)
        )

    def col_pass(copies, p, block, device):
        ref = gcols.at[p, block]
        return remote(ref, ref, copies.send.at[p], copies.recv.at[p], (me, device))

    def send_cols(m):
        col_first(flip(m), me).start()

    loop(1, n_sp, send_cols)
    for k in range(1, bits - 1):
        arrive(k)
        widen(k + 1)
    own_at = pl.ds(pl.multiple_of(me * piece, piece), piece)
    gcols[me] = mid[:, own_at].reshape(n_tp, rows, piece)
    scores_cot = jnp.where(causal, dot(head[...], vv[...].astype(f32), NT, True), 0.0)
    for k in range(1, bits - 1):
        forward_merge(k)
        give(c_fwd, fsend, frecv, ftot, k + 1)
    qc_s[...] = dot(scores_cot, kg_s[...], NN, True)
    reverse_merge(0)
    give(c_rev, usend, urecv, utot, 1)
    loop(0, width // tile, down_grad)
    kc_s[...] = dot(scores_cot, qd_s[...], TN, True)
    gv_s[...] = dot(sc_s[...], head[...], TN, True)
    for k in range(1, bits):
        reverse_merge(k)
        if k < bits - 1:
            give(c_rev, usend, urecv, utot, k + 1)

        if k == 1:
            def col_forward(m):
                p = flip(m)
                col_first(p, p).wait_recv()
                col_pass(d_across, p, tp, far).start()
                col_pass(d_beside, p, tp, near).start()

            loop(1, n_sp, col_forward)
            def col_relay(m):
                p = flip(m)
                col_pass(d_across, p, far, far).wait_recv()
                col_pass(d_relay, p, far, near).start()

            loop(1, n_sp, col_relay)

    forward_merge(bits - 1)
    carry, enter = upre[...], fpre[...]
    qc_s[...] += dot(head[...], enter, NN, True)
    cum = cum_s[...]
    total_decay = cum[tok - 1 : tok, :]
    val = vv[...].astype(f32)
    ke_cot = dot(val, carry, NN, True)
    grad_v[...] = (gv_s[...] + dot(ke_s[...], carry, NT, True)).astype(bf16)
    end = ke_cot * ke_s[...]
    c_cot = qc_s[...] * qd_s[...] - kc_s[...] * kg_s[...] - end
    last = jnp.sum(end, axis=0, keepdims=True) + jnp.exp(total_decay) * jnp.sum(
        carry * enter, axis=0, keepdims=True
    )
    grad_decay[...] = dot(lower, c_cot, TN, True) + last
    grad_q[...] = (qc_s[...] * jnp.exp(cum)).astype(bf16)
    grad_k[...] = (kc_s[...] * jnp.exp(-cum) + ke_cot * jnp.exp(total_decay - cum)).astype(bf16)

    arrive(bits - 1)

    def col_finish(m):
        p = flip(m)
        col_pass(d_beside, p, near, near).wait_recv()
        col_pass(d_relay, p, near_far, near).wait_recv()

    loop(1, n_sp, col_finish)
    grad_proj[...] = dot(
        gcols[...].reshape(n_sp * tok, piece), gmix[...].reshape(n_sp * tok, gmix.shape[2]), TN
    )

    def finish(m):
        p = peer(m)
        decay(p, me).wait_send()
        back(p, me).wait_send()
        col_first(p, me).wait_send()
        col_pass(d_across, p, tp, far).wait_send()
        col_pass(d_beside, p, tp, near).wait_send()
        col_pass(d_relay, p, far, near).wait_send()
        for j in (0, 1):
            first(j, p, me).wait_send()

            @pl.when(m >= close)
            def _():
                across(j, p, tp).wait_send()

            @pl.when(m < close)
            def _():
                second(j, p, me).wait_send()

            beside(j, p, tp).wait_send()
            relay(j, p, far).wait_send()

    loop(1, n_sp, finish)

    def finish_return(m):
        p = flip(m)
        cross(p).wait_send()
        for j in (0, 1):
            half(j, p).wait_send()

    loop(0, n_sp, finish_return)
    for k in range(bits):
        hop(c_fwd, fsend, frecv, k).wait_send()
        hop(c_rev, usend, urecv, k).wait_send()
    spread(0, tp, far).wait_send()
    spread(1, tp, near).wait_send()
    spread(2, far, near).wait_send()


def flush_kernel(*refs):
    count = (len(refs) - 1) // 2
    copies = [
        pltpu.make_async_copy(refs[i], refs[count + i], refs[-1].at[i]) for i in range(count)
    ]
    for copy in copies:
        copy.start()
    for copy in copies:
        copy.wait()


def flush(arrays):
    count = len(arrays)
    return pl.pallas_call(
        flush_kernel,
        out_shape=tuple(jax.ShapeDtypeStruct(a.shape, a.dtype) for a in arrays),
        in_specs=[VM] * count,
        out_specs=(ANY,) * count,
        scratch_shapes=[pltpu.SemaphoreType.DMA((count,))],
        compiler_params=pltpu.CompilerParams(vmem_limit_bytes=1024 * 1024),
    )(*[pltpu.with_memory_space_constraint(a, pltpu.VMEM) for a in arrays])


def whole_plan(*args):
    bf16, f32 = jnp.bfloat16, jnp.float32
    n_sp, n_tp = lax.axis_size("sp"), lax.axis_size("tp")
    expert_in, route_ids, w_gate = args[0], args[2], args[4]
    tok, width = expert_in.shape
    units = w_gate.shape[2]
    cap = 2 * route_ids.shape[1] * tok // n_sp
    share, quarter, piece = cap // n_tp, width // n_tp, width // n_sp
    dv = args[11].shape[1]
    bits = n_sp.bit_length() - 1
    mem = pltpu.VMEM
    held = [
        mem(a.shape[1:] if a.ndim == 3 else a.shape, a.dtype) for a in args[:2] + args[4:]
    ]
    state = (dv, DK)
    scratch = held + [
        mem((tok, tok), f32), mem((tok, tok), f32), mem((tok, n_sp * cap), bf16),
        mem((n_sp, 2, share, width), bf16), mem((n_sp, 2, share, width), bf16),
        mem((n_sp, n_tp, share, width), bf16), mem((n_sp, n_tp, share, width), bf16),
        mem((n_sp, cap, 2 * units), bf16), mem((n_sp, cap, units), bf16), mem((n_sp, cap, width), bf16),
        mem((n_sp, 2, cap, quarter), bf16),
    ] + [mem((n_sp, cap, quarter), bf16)] * 4 + [
        mem((tok, width), bf16), mem((n_sp,) + args[8].shape, bf16), mem((n_sp, n_tp, tok // n_tp, piece), bf16),
        mem((n_sp, 8, DK), f32),
    ] + [mem((bits,) + state, bf16)] * 4 + [mem(state, f32)] * 4 + [mem((tok, dv), f32)] + [
        mem((tok, DK), f32)
    ] * 3 + [mem((tok, tok), f32), mem((tok, DK), f32), mem((tok, DK), f32), mem((tok, dv), f32), mem((tok, DK), f32)]
    scratch += [pltpu.SemaphoreType.DMA((11,)), pltpu.SemaphoreType.DMA]
    scratch += dma(2, n_sp) * 4 + dma(n_sp)
    scratch += [pltpu.SemaphoreType.DMA((bits, n_sp // 2)), pltpu.SemaphoreType.DMA((n_sp,))]
    scratch += dma(bits) + dma(2, n_sp) + dma(n_sp) * 2 + dma(3) + dma(bits) + dma(2, n_sp) + dma(n_sp) * 4
    shapes = [
        ((width, units), f32), ((width, units), f32), ((units, width), f32), ((piece, args[8].shape[1]), f32),
        (args[9].shape, bf16), (args[10].shape, bf16), (args[11].shape, bf16), (args[12].shape, f32),
    ]
    outs = pl.pallas_call(
        functools.partial(whole_kernel, n_sp, n_tp),
        out_shape=tuple(pltpu.VMEM(s, t) for s, t in shapes),
        in_specs=[ANY, ANY, VM, VM] + [ANY] * 9,
        out_specs=(VM,) * 8,
        scratch_shapes=scratch,
        compiler_params=pltpu.CompilerParams(
            collective_id=3, has_side_effects=True, vmem_limit_bytes=56 * 1024 * 1024
        ),
    )(*args[:2], args[2].T, args[3].T, *args[4:])
    outs = flush(outs)
    return tuple(a[None] for a in outs[:3]) + tuple(outs[3:])


def per_device(*args):
    n_sp, n_tp = lax.axis_size("sp"), lax.axis_size("tp")
    tok, top = args[0].shape[0], args[2].shape[1]
    heads = args[9].shape[1] // DK
    share = 2 * top * tok // (n_sp * n_tp)
    aligned = share % 16 == 0 and tok // n_tp % 16 == 0 and tok == 128
    if aligned and heads == 1 and args[4].shape[0] == 1 and n_tp == 4 and n_sp & (n_sp - 1) == 0:
        return whole_plan(*args)
    return spread_plan(*args)


def solution(mesh):
    tokens, both = P("sp", None), P("sp", "tp")
    up, down = P("sp", None, "tp"), P("sp", "tp", None)
    return jax.shard_map(
        per_device,
        mesh=mesh,
        in_specs=(tokens,) * 4 + (up, up, down, P(None, "tp")) + (both,) * 5,
        out_specs=(up, up, down) + (both,) * 5,
        check_vma=False,
    )
```

```python
import functools

import jax
import jax.numpy as jnp
from jax import lax
from jax.experimental import pallas as pl
from jax.experimental.pallas import tpu as pltpu
from jax.sharding import PartitionSpec as P

DK = 128
EXACT = lax.Precision.HIGHEST
MESH = pl.DeviceIdType.MESH


def remote(src, dst, send, recv, device):
    return pltpu.make_async_remote_copy(
        src_ref=src, dst_ref=dst, send_sem=send, recv_sem=recv, device_id=device, device_id_type=MESH
    )


def greet(n_sp, me, tp, partners):
    barrier = pltpu.get_barrier_semaphore()

    def hello(i, carry):
        pl.semaphore_signal(
            barrier, inc=1, device_id=(lax.rem(me + i, n_sp), tp), device_id_type=MESH
        )
        return carry

    lax.fori_loop(1, n_sp, hello, 0)
    for other in partners:
        pl.semaphore_signal(barrier, inc=1, device_id=(me, other), device_id_type=MESH)
    pl.semaphore_wait(barrier, n_sp - 1 + len(partners))


def loop(start, stop, body):
    def step(i, carry):
        body(i)
        return carry

    lax.fori_loop(start, stop, step, 0)


def spread_kernel(n_sp, n_tp, n_rows, n_sides, *refs):
    count = n_rows + n_sides
    given, got = refs[:count], refs[count : 2 * count]
    s0, r0, s1, r1, s2, r2, s3, r3, s4, r4, own_sem = refs[2 * count :]
    me, tp = lax.axis_index("sp"), lax.axis_index("tp")
    far = lax.rem(tp + n_tp // 2, n_tp)
    near = tp + 1 - 2 * lax.rem(tp, 2)
    greet(n_sp, me, tp, (far, near))
    rows = tuple(zip(given[:n_rows], got[:n_rows]))
    sides = tuple(zip(given[n_rows:], got[n_rows:]))

    def first(j, p, slot):
        return remote(rows[j][0].at[p], rows[j][1].at[slot, tp], s0.at[j, p], r0.at[j, slot], (p, tp))

    def across(j, p, share):
        ref = rows[j][1].at[p, share]
        return remote(ref, ref, s1.at[j, p], r1.at[j, p], (me, far))

    def beside(j, p, share):
        ref = rows[j][1].at[p, share]
        return remote(ref, ref, s2.at[j, p], r2.at[j, p], (me, near))

    def relay(j, p, share):
        ref = rows[j][1].at[p, share]
        return remote(ref, ref, s3.at[j, p], r3.at[j, p], (me, near))

    def side(k, p, slot):
        return remote(sides[k][0], sides[k][1].at[slot], s4.at[k, p], r4.at[k, slot], (p, tp))

    def send(i):
        p = lax.rem(me + i, n_sp)
        for j in range(n_rows):
            first(j, p, me).start()

    loop(1, n_sp, send)
    owns = [
        pltpu.make_async_copy(rows[j][0].at[me], rows[j][1].at[me, tp], own_sem.at[j]) for j in range(n_rows)
    ] + [pltpu.make_async_copy(sides[k][0], sides[k][1].at[me], own_sem.at[n_rows + k]) for k in range(n_sides)]
    for own in owns:
        own.start()
    for own in owns:
        own.wait()
    for j in range(n_rows):
        across(j, me, tp).start()
        beside(j, me, tp).start()

    def send_side(i):
        p = lax.rem(me + i, n_sp)
        for k in range(n_sides):
            side(k, p, me).start()

    loop(1, n_sp, send_side)

    def forward(i):
        p = lax.rem(me - i + n_sp, n_sp)
        for j in range(n_rows):
            first(j, p, p).wait_recv()
            across(j, p, tp).start()
            beside(j, p, tp).start()

    loop(1, n_sp, forward)

    def pass_on(i):
        p = lax.rem(me - i + n_sp, n_sp)
        for j in range(n_rows):
            across(j, p, far).wait_recv()
            relay(j, p, far).start()

    loop(0, n_sp, pass_on)
    near_far = lax.rem(near + n_tp // 2, n_tp)

    def finish(i):
        p = lax.rem(me - i + n_sp, n_sp)
        for j in range(n_rows):
            beside(j, p, near).wait_recv()
            relay(j, p, near_far).wait_recv()
            across(j, p, tp).wait_send()
            beside(j, p, tp).wait_send()
            relay(j, p, far).wait_send()

    loop(0, n_sp, finish)

    def finish_side(i):
        p = lax.rem(me - i + n_sp, n_sp)
        for k in range(n_sides):
            side(k, p, p).wait_recv()
            side(k, p, me).wait_send()
        for j in range(n_rows):
            first(j, p, me).wait_send()

    loop(1, n_sp, finish_side)


def return_kernel(
    n_sp, n_tp, part, comb, dy, mix, state, mid, gmix, gstate, in1, out1, in2, out2, ret,
    s1, r1, s2, r2, s3, r3, s4, r4, s5, r5, own_sem,
):
    me, tp = lax.axis_index("sp"), lax.axis_index("tp")
    far = lax.rem(tp + n_tp // 2, n_tp)
    near = tp + 1 - 2 * lax.rem(tp, 2)
    near_far = lax.rem(near + n_tp // 2, n_tp)
    quarter = part.shape[2] // n_tp
    greet(n_sp, me, tp, (far, near))

    gathered = ((mix, gmix), (state, gstate))
    strides = [n_sp >> (k + 1) for k in range(n_sp.bit_length() - 1)]

    def hop(j, k, base, c):
        block = lax.rem(base, 2 * strides[k]) + c * 2 * strides[k]
        partner = me + strides[k] * (1 - 2 * lax.rem(me // strides[k], 2))
        ref = gathered[j][1].at[block]
        return remote(ref, ref, s5.at[j, k, c], r5.at[j, block], (partner, tp))

    def widen(k):
        def one(c):
            for j in (0, 1):
                hop(j, k, me, c).start()

        loop(0, n_sp // (2 * strides[k]), one)

    def arrive(k):
        partner = me + strides[k] * (1 - 2 * lax.rem(me // strides[k], 2))

        def one(c):
            for j in (0, 1):
                hop(j, k, partner, c).wait_recv()
                hop(j, k, me, c).wait_send()

        loop(0, n_sp // (2 * strides[k]), one)

    def columns(block):
        return pl.ds(pl.multiple_of(block * quarter, quarter), quarter)

    def beside(j, p):
        block = near if j == 0 else near_far
        return remote(
            part.at[p, :, columns(block)], in1.at[p, j], s1.at[j, p], r1.at[j, p], (me, near)
        )

    def across(p):
        return remote(out1.at[p], in2.at[p], s2.at[p], r2.at[p], (me, far))

    def back(p, slot):
        return remote(out2.at[p], ret.at[slot], s3.at[p], r3.at[slot], (p, tp))

    def start(i):
        p = lax.rem(me + 1 + i, n_sp)
        for j in (1, 0):
            beside(j, p).start()

    loop(0, n_sp, start)
    owns = [
        pltpu.make_async_copy(gathered[j][0], gathered[j][1].at[me], own_sem.at[j]) for j in (0, 1)
    ]
    for own in owns:
        own.start()
    for own in owns:
        own.wait()
    widen(0)

    def pair(i):
        p = lax.rem(me + 1 + i, n_sp)
        beside(1, p).wait_recv()
        mine = part[p, :, columns(far)].astype(jnp.float32)
        out1[p] = (mine + in1[p, 1].astype(jnp.float32)).astype(jnp.bfloat16)
        across(p).start()

    loop(0, n_sp, pair)
    arrive(0)
    for k in range(1, len(strides) - 1):
        widen(k)
        arrive(k)

    def total(p):
        beside(0, p).wait_recv()
        across(p).wait_recv()
        mine = part[p, :, columns(tp)].astype(jnp.float32)
        mine = mine + in1[p, 0].astype(jnp.float32)
        return (mine + in2[p].astype(jnp.float32)).astype(jnp.bfloat16)

    def quad(i):
        p = lax.rem(me + i, n_sp)
        out2[p] = total(p)
        back(p, me).start()

    loop(1, n_sp, quad)
    ret[me] = total(me)
    widen(len(strides) - 1)

    def gather(i, acc):
        p = lax.rem(me - i + n_sp, n_sp)

        @pl.when(i > 0)
        def _():
            back(p, p).wait_recv()

        return acc + jnp.dot(comb[p], ret[p], preferred_element_type=jnp.float32)

    acc = lax.fori_loop(0, n_sp, gather, dy[:, columns(tp)].astype(jnp.float32))
    mid[:, columns(tp)] = acc.astype(jnp.bfloat16)

    def share(k, block, device):
        ref = mid.at[:, columns(block)]
        return remote(ref, ref, s4.at[k], r4.at[k], (me, device))

    share(0, tp, far).start()
    share(1, tp, near).start()
    share(0, far, far).wait_recv()
    share(2, far, near).start()
    share(1, near, near).wait_recv()
    share(2, near_far, near).wait_recv()
    share(0, tp, far).wait_send()
    share(1, tp, near).wait_send()
    share(2, far, near).wait_send()

    arrive(len(strides) - 1)

    def finish(i):
        p = lax.rem(me + i, n_sp)
        for j in (0, 1):
            beside(j, p).wait_send()
        across(p).wait_send()

        @pl.when(i > 0)
        def _():
            back(p, me).wait_send()

    loop(0, n_sp, finish)


VM = pl.BlockSpec(memory_space=pltpu.VMEM)
ANY = pl.BlockSpec(memory_space=pl.ANY)


def dma(*shape):
    return [pltpu.SemaphoreType.DMA(shape), pltpu.SemaphoreType.DMA(shape)]


def call(kernel, ident, operands, in_specs, out_shape, out_specs, scratch):
    return pl.pallas_call(
        kernel,
        out_shape=out_shape,
        in_specs=in_specs,
        out_specs=out_specs,
        scratch_shapes=scratch,
        compiler_params=pltpu.CompilerParams(
            collective_id=ident, has_side_effects=True, vmem_limit_bytes=48 * 1024 * 1024
        ),
    )(*operands)


def spread_plan(
    expert_in, out_cot, route_ids, route_weights, w_gate, w_up, w_down, w_out,
    mixed_heads, queries, keys, values, log_decay,
):
    bf16, f32 = jnp.bfloat16, jnp.float32
    n_sp, n_tp = lax.axis_size("sp"), lax.axis_size("tp")
    me, tp = lax.axis_index("sp"), lax.axis_index("tp")
    tok, width = expert_in.shape
    top = route_ids.shape[1]
    experts = w_gate.shape[0] * n_sp
    cap = 2 * top * tok // experts
    share = cap // n_tp

    ids = route_ids.reshape(-1)
    onehot = ids[:, None] == jnp.arange(experts, dtype=jnp.int32)
    order = jnp.arange(tok * top, dtype=jnp.int32)
    below = (order[None, :] < order[:, None]).astype(bf16)
    ranks = jnp.dot(below, onehot.astype(bf16), preferred_element_type=f32)
    rank = jnp.sum(jnp.where(onehot, ranks, 0.0), axis=1).astype(jnp.int32)
    slot = (ids * cap + rank).reshape(tok, top)
    mine = (
        jnp.arange(experts, dtype=jnp.int32)[:, None] * cap
        + tp * share
        + jnp.arange(share, dtype=jnp.int32)[None, :]
    ).reshape(-1)
    match = slot[None] == mine[:, None, None]
    pick = jnp.any(match, axis=2).astype(bf16)
    slot_weight = jnp.sum(jnp.where(match, route_weights[None], 0.0), axis=(1, 2))
    x_share = jnp.dot(pick, expert_in, preferred_element_type=f32).astype(bf16)
    dy_share = (
        slot_weight[:, None] * jnp.dot(pick, out_cot, preferred_element_type=f32)
    ).astype(bf16)
    places = jnp.arange(experts * cap, dtype=jnp.int32).reshape(experts, 1, cap, 1)
    comb = jnp.any(slot[None, :, None, :] == places, axis=3).astype(bf16)

    heads = queries.shape[1] // DK
    dv = values.shape[1] // heads
    step = jnp.arange(tok, dtype=jnp.int32)
    causal = step[None, :] <= step[:, None]
    lower = causal.astype(f32)
    cumulative = jnp.dot(lower, log_decay, precision=EXACT)
    decay_sum = cumulative[-1:]

    def split(array):
        return array.astype(f32).reshape(tok, heads, -1)

    q, k, v = split(queries), split(keys), split(values)
    grow, shrink, to_end = (
        split(jnp.exp(-cumulative)),
        split(jnp.exp(cumulative)),
        split(jnp.exp(decay_sum - cumulative)),
    )
    qd, kg, ke = q * shrink, k * grow, k * to_end
    state_local = jnp.einsum("thd,the->hde", ke, v, precision=EXACT)

    rows = jax.ShapeDtypeStruct((n_sp, n_tp, share, width), bf16)
    gx, gdy, gdecay = call(
        functools.partial(spread_kernel, n_sp, n_tp, 2, 1),
        0,
        (
            x_share.reshape(n_sp, share, width),
            dy_share.reshape(n_sp, share, width),
            decay_sum,
        ),
        [VM] * 3,
        (
            rows,
            rows,
            jax.ShapeDtypeStruct((n_sp,) + decay_sum.shape, f32),
        ),
        (ANY, ANY, ANY),
        dma(2, n_sp) * 4 + dma(1, n_sp) + [pltpu.SemaphoreType.DMA((3,))],
    )
    got_x = gx.reshape(n_sp * cap, width)
    got_dy = gdy.reshape(n_sp * cap, width)
    wg, wu, wd = w_gate[0], w_up[0], w_down[0]
    gate_pre = jnp.dot(got_x, wg, preferred_element_type=f32)
    up_pre = jnp.dot(got_x, wu, preferred_element_type=f32)
    hidden_cot = lax.dot_general(got_dy, wd, (((1,), (1,)), ((), ())), preferred_element_type=f32)
    sig = jax.nn.sigmoid(gate_pre)
    hidden = (gate_pre * sig * up_pre).astype(bf16)
    gate_cot = (hidden_cot * up_pre * sig * (1.0 + gate_pre * (1.0 - sig))).astype(bf16)
    up_cot = (hidden_cot * gate_pre * sig).astype(bf16)
    back = (((1,), (1,)), ((), ()))
    part = lax.dot_general(gate_cot, wg, back, preferred_element_type=f32) + lax.dot_general(
        up_cot, wu, back, preferred_element_type=f32
    )
    part = part.astype(bf16).reshape(n_sp, cap, width)
    over = (((0,), (0,)), ((), ()))
    grad_gate = lax.dot_general(got_x, gate_cot, over, preferred_element_type=f32)[None]
    grad_up = lax.dot_general(got_x, up_cot, over, preferred_element_type=f32)[None]
    grad_down = lax.dot_general(hidden, got_dy, over, preferred_element_type=f32)[None]

    quarter = width // n_tp
    buf = pltpu.VMEM((n_sp, cap, quarter), bf16)
    mid, gmix, gstate = call(
        functools.partial(return_kernel, n_sp, n_tp),
        1,
        (part, comb, out_cot, mixed_heads, state_local.reshape(heads * DK, dv).astype(bf16)),
        [VM] * 5,
        (
            jax.ShapeDtypeStruct((tok, width), bf16),
            jax.ShapeDtypeStruct((n_sp,) + mixed_heads.shape, bf16),
            jax.ShapeDtypeStruct((n_sp, heads * DK, dv), bf16),
        ),
        (VM, VM, VM),
        [pltpu.VMEM((n_sp, 2, cap, quarter), bf16), buf, buf, buf, buf]
        + dma(2, n_sp) + dma(n_sp) + dma(n_sp) + dma(3)
        + [
            pltpu.SemaphoreType.DMA((2, n_sp.bit_length() - 1, n_sp // 2)),
            pltpu.SemaphoreType.DMA((2, n_sp)),
            pltpu.SemaphoreType.DMA((2,)),
        ],
    )
    head_cot = split(jnp.dot(mid, w_out, preferred_element_type=f32))
    pull = jnp.einsum("thd,the->hde", qd, head_cot, precision=EXACT)
    part_tok = tok // n_tp
    cols = lax.dynamic_slice_in_dim(mid, tp * part_tok, part_tok, 0)
    cols = cols.reshape(part_tok, n_sp, width // n_sp).swapaxes(0, 1)
    gcols, gpull = call(
        functools.partial(spread_kernel, n_sp, n_tp, 1, 1),
        2,
        (cols, pull.reshape(heads * DK, dv).astype(bf16)),
        [VM] * 2,
        (
            jax.ShapeDtypeStruct((n_sp, n_tp, part_tok, width // n_sp), bf16),
            jax.ShapeDtypeStruct((n_sp, heads * DK, dv), bf16),
        ),
        (VM, VM),
        dma(1, n_sp) * 5 + [pltpu.SemaphoreType.DMA((2,))],
    )
    gcols = gcols.reshape(n_sp, tok, width // n_sp)
    grad_out_proj = jnp.einsum("ntd,nte->de", gcols, gmix, preferred_element_type=f32)

    sums = gdecay[:, 0]
    index = jnp.arange(n_sp, dtype=jnp.int32)
    between = (index[None] > jnp.minimum(index, me)[:, None]) & (
        index[None] < jnp.maximum(index, me)[:, None]
    )
    weight = jnp.exp(jnp.sum(jnp.where(between[..., None], sums[None], 0.0), axis=1))

    def entering(pieces, used):
        scale = jnp.where(used[:, None], weight, 0.0)
        return jnp.sum(scale[..., None] * pieces.astype(f32), axis=0).reshape(heads, DK, dv)

    state_in = entering(gstate, index < me)
    state_cot = entering(gpull, index > me)

    dot = functools.partial(jnp.einsum, precision=EXACT)
    scores = jnp.where(causal, dot("thd,shd->hts", qd, kg), 0.0)
    scores_cot = jnp.where(causal, dot("the,she->hts", head_cot, v), 0.0)
    grad_v = dot("hts,the->she", scores, head_cot) + dot("shd,hde->she", ke, state_cot)
    qd_cot = dot("hts,shd->thd", scores_cot, kg) + dot("the,hde->thd", head_cot, state_in)
    kg_cot = dot("hts,thd->shd", scores_cot, qd)
    ke_cot = dot("she,hde->shd", v, state_cot)
    end = ke_cot * ke
    c_cot = (qd_cot * qd - kg_cot * kg - end).reshape(tok, heads * DK)
    last = jnp.sum(end, axis=0).reshape(-1) + jnp.exp(decay_sum[0]) * jnp.sum(
        state_cot * state_in, axis=2
    ).reshape(-1)
    grad_decay = lax.dot_general(lower, c_cot, over, precision=EXACT) + last[None]
    grad_q = (qd_cot * shrink).astype(bf16).reshape(tok, heads * DK)
    grad_k = (kg_cot * grow + ke_cot * to_end).astype(bf16).reshape(tok, heads * DK)
    return (
        grad_gate,
        grad_up,
        grad_down,
        grad_out_proj,
        grad_q,
        grad_k,
        grad_v.astype(bf16).reshape(tok, heads * dv),
        grad_decay,
    )


class Copies:
    def __init__(self, send, recv):
        self.send, self.recv = send, recv


def dot(a, b, dims, exact=False):
    return lax.dot_general(
        a, b, (dims, ((), ())), precision=EXACT if exact else None, preferred_element_type=jnp.float32
    )


NN, NT, TN = ((1,), (0,)), ((1,), (1,)), ((0,), (0,))


def whole_kernel(n_sp, n_tp, *refs):
    bf16, f32 = jnp.bfloat16, jnp.float32
    given, refs = refs[:13], refs[13:]
    outs, refs = refs[:8], refs[8:]
    x_hbm, dy_hbm, ids, weights, *_ = given
    out_gate, out_up, out_down, grad_proj, grad_q, grad_k, grad_v, grad_decay = outs
    (
        x_in, dy_in, wg, wu, wd, wo, mixed, qv, kv, vv, gv,
        pos_t, wt, comb, xs, dys, gx, gdy, cots, hid, part, in1, out1, in2, out2, ret,
        mid, gmix, gcols, dall, fsend, frecv, usend, urecv, ftot, fpre, utot, upre,
        head, qd_s, kg_s, ke_s, sc_s, qc_s, kc_s, gv_s, cum_s,
        grad_gate, grad_up, grad_down, load, own_sem, put_sem, *sems,
    ) = refs
    pairs = [Copies(a, b) for a, b in zip(sems[::2], sems[1::2])]
    (
        c_first, c_across, c_beside, c_relay, c_sum, c_mix, c_fwd, c_half, c_cross, c_back,
        c_share, c_rev, d_first, d_across, d_beside, d_relay,
    ) = pairs
    me, tp = lax.axis_index("sp"), lax.axis_index("tp")
    far = lax.rem(tp + n_tp // 2, n_tp)
    near = tp + 1 - 2 * lax.rem(tp, 2)
    near_far = lax.rem(near + n_tp // 2, n_tp)
    tok, width = x_in.shape
    share = xs.shape[1]
    cap = share * n_tp
    quarter = width // n_tp
    piece = width // n_sp
    rows = tok // n_tp
    bits = n_sp.bit_length() - 1

    sources = (x_hbm, dy_hbm) + tuple(given[4:])
    places = (x_in, dy_in, wg, wu, wd, wo, mixed, qv, kv, vv, gv)

    def fetch(i):
        src = sources[i].at[0] if len(sources[i].shape) == 3 else sources[i]
        return pltpu.make_async_copy(src, places[i], load.at[i])

    for i in range(len(places)):
        fetch(i).start()

    barrier = pltpu.get_barrier_semaphore()

    def hello(i):
        pl.semaphore_signal(
            barrier, inc=1, device_id=(lax.rem(me + i, n_sp), tp), device_id_type=MESH
        )

    loop(1, n_sp, hello)
    for other in (far, near):
        pl.semaphore_signal(barrier, inc=1, device_id=(me, other), device_id_type=MESH)

    def flip(m):
        out = 0
        for b in range(bits):
            a, c = lax.rem(me // (1 << b), 2), lax.rem(m // (1 << b), 2)
            out = out + (1 << b) * (a + c - 2 * a * c)
        return out

    def turn(i):
        zero = 1 - (i + n_sp - 1) // n_sp
        is_near = lax.rem(i, 2) * (1 - i // (n_sp - 1)) + zero
        half_way = (i + 1) // 2
        return half_way + (1 - is_near) * (n_sp // 2 - 1)

    def peer(i):
        return flip(turn(i))

    others = pl.ds(0, n_sp - 1)

    def whole(copies, ref):
        recv = copies.recv.at[(0,) * len(copies.recv.shape)] if copies.recv.shape else copies.recv
        return remote(ref, ref, copies.send, recv, (me, far))

    def got_all(copies, ref):
        whole(copies, ref).wait_recv()

    def columns(block):
        return pl.ds(pl.multiple_of(block * quarter, quarter), quarter)

    down = lax.broadcasted_iota(jnp.int32, (tok, tok), 0)
    across_i = lax.broadcasted_iota(jnp.int32, (tok, tok), 1)
    weight, hit = jnp.zeros((tok, tok), f32), jnp.zeros((tok, tok), f32)
    for j in range(ids.shape[0]):
        hit_j = ids[j : j + 1, :] == down
        weight = weight + jnp.where(hit_j, weights[j : j + 1, :], 0.0)
        hit = hit + jnp.where(hit_j, 1.0, 0.0)
    above = jnp.where(down < across_i, 1.0, 0.0).astype(bf16)
    pos = jnp.where(hit > 0.5, dot(hit.astype(bf16), above, NN), -1.0)
    pos_t[...] = pos
    wt[...] = weight
    pos = jnp.transpose(pos)
    slot_lane = lax.broadcasted_iota(jnp.int32, (tok, cap), 1).astype(f32)
    for e in range(n_sp):
        comb[:, e * cap : (e + 1) * cap] = jnp.where(pos[:, e : e + 1] == slot_lane, 1.0, 0.0).astype(bf16)

    fetch(0).wait()
    fetch(1).wait()

    def chosen(e, start, count):
        want = (lax.broadcasted_iota(jnp.int32, (count, tok), 0) + start).astype(f32)
        match = pos_t[pl.ds(e, 1), :] == want
        scale = jnp.sum(jnp.where(match, wt[pl.ds(e, 1), :], 0.0), axis=1, keepdims=True)
        return jnp.where(match, 1.0, 0.0), scale

    found = [chosen(e, tp * share, share) for e in range(n_sp)]
    pick = jnp.concatenate([a for a, _ in found], axis=0).astype(bf16)
    scale = jnp.concatenate([b for _, b in found], axis=0)
    xs[...] = dot(pick, x_in[...], NN).astype(bf16).reshape(n_sp, share, width)
    dys[...] = (scale * dot(pick, dy_in[...], NN)).astype(bf16).reshape(n_sp, share, width)

    pl.semaphore_wait(barrier, n_sp + 1)

    row_pairs = ((xs, gx), (dys, gdy))

    def first(j, p, slot):
        return remote(
            row_pairs[j][0].at[p], row_pairs[j][1].at[slot, tp],
            c_first.send, c_first.recv.at[j, slot], (p, tp),
        )

    def passing(copies, j, p, block, device):
        ref = row_pairs[j][1].at[p, block]
        return remote(ref, ref, copies.send, copies.recv.at[p], (me, device))

    def arrived(copies, p):
        ref = gx.at[p, pl.ds(0, 2)]
        remote(ref, ref, copies.send, copies.recv.at[p], (me, far)).wait_recv()

    def across(j, p, block):
        return passing(c_across, j, p, block, far)

    def beside(j, p, block):
        return passing(c_beside, j, p, block, near)

    def relay(j, p, block):
        return passing(c_relay, j, p, block, near)

    def dispatch(m):
        p = peer(m)
        for j in (0, 1):
            first(j, p, me).start()

    loop(1, n_sp, dispatch)

    own_pick, own_scale = chosen(me, 0, cap)
    own_pick = own_pick.astype(bf16)
    gx[me] = dot(own_pick, x_in[...], NN).astype(bf16).reshape(n_tp, share, width)
    gdy[me] = (own_scale * dot(own_pick, dy_in[...], NN)).astype(bf16).reshape(n_tp, share, width)

    for i in range(6, 11):
        fetch(i).wait()
    causal = across_i <= down
    lower = jnp.where(causal, 1.0, 0.0)
    cum = dot(lower, gv[...], NN, True)
    total_decay = cum[tok - 1 : tok, :]
    cum_s[...] = cum
    dall[me] = jnp.broadcast_to(total_decay, dall.shape[1:])

    def decay(p, slot):
        return remote(dall.at[me], dall.at[slot], c_sum.send, c_sum.recv, (p, tp))

    def send_decay(m):
        decay(flip(m), me).start()

    loop(1, n_sp, send_decay)
    key = kv[...].astype(f32)
    val = vv[...].astype(f32)
    qd_s[...] = qv[...].astype(f32) * jnp.exp(cum)
    kg_s[...] = key * jnp.exp(-cum)
    ke_s[...] = key * jnp.exp(total_decay - cum)
    ftot[...] = dot(val, ke_s[...], TN, True)
    fpre[...] = jnp.zeros_like(fpre)

    piece_rows = ftot.shape[0] // 2

    def hop(copies, held, got, k, c):
        partner = me + (1 << k) * (1 - 2 * lax.rem(me // (1 << k), 2))
        return remote(held.at[k, c], got.at[k, c], copies.send, copies.recv.at[k, c], (partner, tp))

    def lines(c):
        return slice(c * piece_rows, (c + 1) * piece_rows)

    def give(copies, held, got, total, k, c):
        held[k, c] = total[lines(c), :].astype(bf16)
        hop(copies, held, got, k, c).start()

    def decay_over(low, high):
        table = dall[:, 0, :]
        index = lax.broadcasted_iota(jnp.int32, table.shape, 0)
        picked = jnp.where((index >= low) & (index < high), table, 0.0)
        return jnp.exp(jnp.sum(picked, axis=0, keepdims=True))

    def span(k):
        size = 1 << k
        base = me - lax.rem(me, size)
        upper = lax.rem(me // size, 2)
        return base, base + size, upper

    def forward_merge(k, c):
        hop(c_fwd, fsend, frecv, k, c).wait_recv()
        low, high, upper = span(k)
        got = frecv[k, c].astype(f32)
        is_upper = upper == 1
        at = lines(c)
        fpre[at, :] = fpre[at, :] + jnp.where(is_upper, decay_over(low, me), 0.0) * got
        mine = jnp.where(is_upper, 1.0, decay_over(low + (1 << k), high + (1 << k)))
        theirs = jnp.where(is_upper, decay_over(low, high), 1.0)
        ftot[at, :] = mine * ftot[at, :] + theirs * got

    def reverse_merge(k, c):
        low, high, upper = span(k)
        is_upper = upper == 1
        after = jnp.where(is_upper, 0.0, decay_over(me + 1, high))
        mine = jnp.where(is_upper, decay_over(low - (1 << k), low), 1.0)
        theirs = jnp.where(is_upper, 1.0, decay_over(low, high))
        hop(c_rev, usend, urecv, k, c).wait_recv()
        got = urecv[k, c].astype(f32)
        at = lines(c)
        if k < bits - 1:
            utot[at, :] = mine * utot[at, :] + theirs * got
            give(c_rev, usend, urecv, utot, k + 1, c)
        upre[at, :] = upre[at, :] + after * got

    strides = [n_sp >> (k + 1) for k in range(bits)]

    def mix_hop(k, base, c):
        block = lax.rem(base, 2 * strides[k]) + c * 2 * strides[k]
        block = lax.rem(block, n_sp)
        partner = me + strides[k] * (1 - 2 * lax.rem(me // strides[k], 2))
        ref = gmix.at[block]
        return remote(ref, ref, c_mix.send, c_mix.recv.at[block], (partner, tp))

    def widen(k):
        def one(c):
            mix_hop(k, me, c).start()

        loop(0, n_sp // (2 * strides[k]), one)

    def arrive(k):
        partner = me + strides[k] * (1 - 2 * lax.rem(me // strides[k], 2))

        def one(c):
            mix_hop(k, partner, c).wait_recv()

        loop(0, n_sp // (2 * strides[k]), one)

    own_mix = pltpu.make_async_copy(mixed, gmix.at[me], own_sem)
    own_mix.start()
    own_mix.wait()
    widen(0)
    for c in (0, 1):
        give(c_fwd, fsend, frecv, ftot, 0, c)
    sc_s[...] = jnp.where(causal, dot(qd_s[...], kg_s[...], NT, True), 0.0)
    for i in range(2, 6):
        fetch(i).wait()

    def half(j, p):
        block = near if j == 0 else near_far
        return remote(
            part.at[p, :, columns(block)], in1.at[p, j], c_half.send, c_half.recv.at[j, p], (me, near)
        )

    def cross(p):
        return remote(out1.at[p], in2.at[p], c_cross.send, c_cross.recv.at[p], (me, far))

    def back(p, slot):
        return remote(out2.at[p], ret.at[slot], c_back.send, c_back.recv, (p, tp))

    def expert(m):
        p = peer(m)

        @pl.when(m > 0)
        def _():
            arrived(c_beside, p)
            arrived(c_relay, p)

        x = gx[p].reshape(cap, width)
        dy = gdy[p].reshape(cap, width)
        gate = dot(x, wg[...], NN)
        up = dot(x, wu[...], NN)
        hidden_cot = dot(dy, wd[...], NT)
        sig = jax.nn.sigmoid(gate)
        hid[p] = (gate * sig * up).astype(bf16)
        gate_cot = (hidden_cot * up * sig * (1.0 + gate * (1.0 - sig))).astype(bf16)
        up_cot = (hidden_cot * gate * sig).astype(bf16)
        units = gate_cot.shape[1]
        cots[p, :, :units] = gate_cot
        cots[p, :, units:] = up_cot
        part[p] = (dot(gate_cot, wg[...], NT) + dot(up_cot, wu[...], NT)).astype(bf16)
        for j in (1, 0):
            half(j, p).start()

    def step(i):
        @pl.when((i >= 3) & (i < n_sp + 3))
        def _():
            p = peer(i - 3)
            half(1, p).wait_recv()
            mine = part[p, :, columns(far)].astype(f32)
            out1[p] = (mine + in1[p, 1].astype(f32)).astype(bf16)
            cross(p).start()

        @pl.when(i < n_sp)
        def _():
            p = peer(i)
            for j in (0, 1):
                first(j, p, p).wait_recv()
                across(j, p, tp).start()
                beside(j, p, tp).start()

        @pl.when((i >= 3) & (i < n_sp + 2))
        def _():
            expert(i - 2)

        @pl.when((i >= 2) & (i < n_sp + 1))
        def _():
            p = peer(i - 1)
            arrived(c_across, p)
            for j in (0, 1):
                relay(j, p, far).start()

        @pl.when(i >= 4)
        def _():
            p = peer(i - 4)
            half(0, p).wait_recv()
            cross(p).wait_recv()
            mine = part[p, :, columns(tp)].astype(f32)
            mine = mine + in1[p, 0].astype(f32)
            out2[p] = (mine + in2[p].astype(f32)).astype(bf16)

            @pl.when(i > 4)
            def _():
                back(p, me).start()

    expert(0)
    loop(1, n_sp, step)
    arrive(0)
    widen(1)
    loop(n_sp, n_sp + 2, step)
    for n in range(1, bits - 1):
        arrive(n)
        widen(n + 1)
    loop(n_sp + 2, n_sp + 4, step)
    ret[me] = out2[me]

    all_x = gx.reshape(n_sp * cap, width)
    all_dy = gdy.reshape(n_sp * cap, width)
    tile = 256

    def weight_grad(b):
        at = pl.ds(pl.multiple_of(b * tile, tile), tile)
        both = cots[...].reshape(n_sp * cap, cots.shape[2])
        units = cots.shape[2] // 2
        grads = dot(all_x[:, at], both, TN)
        grad_gate[at, :] = grads[:, :units]
        grad_up[at, :] = grads[:, units:]

    def down_grad(b):
        at = pl.ds(pl.multiple_of(b * tile, tile), tile)
        grad_down[:, at] = dot(hid[...].reshape(n_sp * cap, hid.shape[2]), all_dy[:, at], TN)

    def put(i):
        src = (grad_gate, grad_up, grad_down)[i]
        return pltpu.make_async_copy(src, (out_gate, out_up, out_down)[i], put_sem.at[i])

    loop(0, width // tile, down_grad)
    put(2).start()
    got_all(c_back, ret.at[others])
    acc = dot(comb[...], ret[...].reshape(n_sp * cap, quarter), NN)
    mid[:, columns(tp)] = (acc + dy_in[:, columns(tp)].astype(f32)).astype(bf16)

    def spread(k, block, device):
        ref = mid.at[:, columns(block)]
        return remote(ref, ref, c_share.send, c_share.recv.at[k], (me, device))

    def project(block):
        at = pl.ds(pl.multiple_of(block * quarter, quarter), quarter)
        return dot(mid[:, columns(block)], wo[at, :], NN)

    spread(0, tp, far).start()
    spread(1, tp, near).start()
    got_all(c_sum, dall.at[others])
    for c in (0, 1):
        forward_merge(0, c)
        give(c_fwd, fsend, frecv, ftot, 1, c)
    head[...] = project(tp)
    spread(1, near, near).wait_recv()
    head[...] += project(near)
    spread(0, far, far).wait_recv()
    spread(2, far, near).start()
    head[...] += project(far)
    spread(2, near_far, near).wait_recv()
    head[...] += project(near_far)

    utot[...] = dot(head[...], qd_s[...], TN, True)
    upre[...] = jnp.zeros_like(upre)
    for c in (0, 1):
        give(c_rev, usend, urecv, utot, 0, c)

    def col_first(p, slot):
        at = pl.ds(pl.multiple_of(p * piece, piece), piece)
        mine = pl.ds(pl.multiple_of(tp * rows, rows), rows)
        return remote(
            mid.at[mine, at], gcols.at[slot, tp], d_first.send, d_first.recv, (p, tp)
        )

    def col_pass(copies, p, block, device):
        ref = gcols.at[p, block]
        return remote(ref, ref, copies.send, copies.recv, (me, device))

    def send_cols(m):
        col_first(flip(m), me).start()

    loop(1, n_sp, send_cols)
    own_at = pl.ds(pl.multiple_of(me * piece, piece), piece)
    gcols[me] = mid[:, own_at].reshape(n_tp, rows, piece)
    scores_cot = jnp.where(causal, dot(head[...], vv[...].astype(f32), NT, True), 0.0)
    for k in range(1, bits - 1):
        for c in (0, 1):
            forward_merge(k, c)
            give(c_fwd, fsend, frecv, ftot, k + 1, c)
    qc_s[...] = dot(scores_cot, kg_s[...], NN, True)
    kc_s[...] = dot(scores_cot, qd_s[...], TN, True)
    gv_s[...] = dot(sc_s[...], head[...], TN, True)

    def col_forward():
        got_all(d_first, gcols.at[others, 0])

        def one(m):
            p = flip(m)
            col_pass(d_across, p, tp, far).start()
            col_pass(d_beside, p, tp, near).start()

        loop(1, n_sp, one)

    def col_relay():
        got_all(d_across, gcols.at[others, 0])

        def one(m):
            col_pass(d_relay, flip(m), far, near).start()

        loop(1, n_sp, one)

    steps = width // tile
    for k in range(bits - 1):
        loop(steps * k // (bits - 1), steps * (k + 1) // (bits - 1), weight_grad)
        if k == bits - 2:
            put(0).start()
            put(1).start()
            pl.when(me < n_sp // 2)(col_forward)
        for c in (0, 1):
            reverse_merge(k, c)
    pl.when(me >= n_sp // 2)(col_forward)
    col_relay()
    for c in (0, 1):
        reverse_merge(bits - 1, c)
    for c in (0, 1):
        forward_merge(bits - 1, c)
    carry, enter = upre[...], fpre[...]
    qc_s[...] += dot(head[...], enter, NN, True)
    cum = cum_s[...]
    total_decay = cum[tok - 1 : tok, :]
    val = vv[...].astype(f32)
    ke_cot = dot(val, carry, NN, True)
    grad_v[...] = (gv_s[...] + dot(ke_s[...], carry, NT, True)).astype(bf16)
    end = ke_cot * ke_s[...]
    c_cot = qc_s[...] * qd_s[...] - kc_s[...] * kg_s[...] - end
    last = jnp.sum(end, axis=0, keepdims=True) + jnp.exp(total_decay) * jnp.sum(
        carry * enter, axis=0, keepdims=True
    )
    grad_decay[...] = dot(lower, c_cot, TN, True) + last
    grad_q[...] = (qc_s[...] * jnp.exp(cum)).astype(bf16)
    grad_k[...] = (kc_s[...] * jnp.exp(-cum) + ke_cot * jnp.exp(total_decay - cum)).astype(bf16)

    arrive(bits - 1)

    got_all(d_beside, gcols.at[others, 0])
    got_all(d_relay, gcols.at[others, 0])
    grad_proj[...] = dot(
        gcols[...].reshape(n_sp * tok, piece), gmix[...].reshape(n_sp * tok, gmix.shape[2]), TN
    )

    def sent(copies, ref):
        whole(copies, ref).wait_send()

    for copies in (c_first, c_across, c_beside, c_relay):
        sent(copies, gx.at[others, pl.ds(0, 2)])
    for copies in (d_first, d_across, d_beside, d_relay):
        sent(copies, gcols.at[others, 0])
    sent(c_sum, dall.at[others])
    sent(c_mix, gmix.at[others])
    sent(c_fwd, fsend)
    sent(c_rev, usend)
    sent(c_half, in1)
    sent(c_cross, out1)
    sent(c_back, out2.at[others])
    sent(c_share, mid.at[:, pl.ds(0, 3 * quarter)])
    for i in range(3):
        put(i).wait()


def flush_kernel(*refs):
    count = (len(refs) - 1) // 2
    copies = [
        pltpu.make_async_copy(refs[i], refs[count + i], refs[-1].at[i]) for i in range(count)
    ]
    for copy in copies:
        copy.start()
    for copy in copies:
        copy.wait()


def flush(arrays):
    count = len(arrays)
    return pl.pallas_call(
        flush_kernel,
        out_shape=tuple(jax.ShapeDtypeStruct(a.shape, a.dtype) for a in arrays),
        in_specs=[VM] * count,
        out_specs=(ANY,) * count,
        scratch_shapes=[pltpu.SemaphoreType.DMA((count,))],
        compiler_params=pltpu.CompilerParams(vmem_limit_bytes=1024 * 1024),
    )(*[pltpu.with_memory_space_constraint(a, pltpu.VMEM) for a in arrays])


def whole_plan(*args):
    bf16, f32 = jnp.bfloat16, jnp.float32
    n_sp, n_tp = lax.axis_size("sp"), lax.axis_size("tp")
    expert_in, route_ids, w_gate = args[0], args[2], args[4]
    tok, width = expert_in.shape
    units = w_gate.shape[2]
    cap = 2 * route_ids.shape[1] * tok // n_sp
    share, quarter, piece = cap // n_tp, width // n_tp, width // n_sp
    dv = args[11].shape[1]
    bits = n_sp.bit_length() - 1
    mem = pltpu.VMEM
    held = [
        mem(a.shape[1:] if a.ndim == 3 else a.shape, a.dtype) for a in args[:2] + args[4:]
    ]
    state = (dv, DK)
    scratch = held + [
        mem((tok, tok), f32), mem((tok, tok), f32), mem((tok, n_sp * cap), bf16),
        mem((n_sp, share, width), bf16), mem((n_sp, share, width), bf16),
        mem((n_sp, n_tp, share, width), bf16), mem((n_sp, n_tp, share, width), bf16),
        mem((n_sp, cap, 2 * units), bf16), mem((n_sp, cap, units), bf16), mem((n_sp, cap, width), bf16),
        mem((n_sp, 2, cap, quarter), bf16),
    ] + [mem((n_sp, cap, quarter), bf16)] * 4 + [
        mem((tok, width), bf16), mem((n_sp,) + args[8].shape, bf16), mem((n_sp, n_tp, tok // n_tp, piece), bf16),
        mem((n_sp, 8, DK), f32),
    ] + [mem((bits, 2, dv // 2, DK), bf16)] * 4 + [mem(state, f32)] * 4 + [mem((tok, dv), f32)] + [
        mem((tok, DK), f32)
    ] * 3 + [mem((tok, tok), f32), mem((tok, DK), f32), mem((tok, DK), f32), mem((tok, dv), f32), mem((tok, DK), f32)]
    scratch += [mem((width, units), f32)] * 2 + [mem((units, width), f32)]
    scratch += [pltpu.SemaphoreType.DMA((11,)), pltpu.SemaphoreType.DMA, pltpu.SemaphoreType.DMA((3,))]
    one = pltpu.SemaphoreType.DMA
    counts = [(2, n_sp)] + [(n_sp,)] * 3 + [(), (n_sp,)] + [(bits, 2), (2, n_sp), (n_sp,), (), (3,), (bits, 2)] + [()] * 4
    for count in counts:
        scratch += [one, one(count) if count else one]
    shapes = [
        ((width, units), f32), ((width, units), f32), ((units, width), f32), ((piece, args[8].shape[1]), f32),
        (args[9].shape, bf16), (args[10].shape, bf16), (args[11].shape, bf16), (args[12].shape, f32),
    ]
    outs = pl.pallas_call(
        functools.partial(whole_kernel, n_sp, n_tp),
        out_shape=tuple(pltpu.VMEM(s, t) for s, t in shapes),
        in_specs=[ANY, ANY, VM, VM] + [ANY] * 9,
        out_specs=(ANY,) * 3 + (VM,) * 5,
        scratch_shapes=scratch,
        compiler_params=pltpu.CompilerParams(
            collective_id=3, has_side_effects=True, vmem_limit_bytes=56 * 1024 * 1024
        ),
    )(*args[:2], args[2].T, args[3].T, *args[4:])
    outs = flush(outs)
    return tuple(a[None] for a in outs[:3]) + tuple(outs[3:])


def per_device(*args):
    n_sp, n_tp = lax.axis_size("sp"), lax.axis_size("tp")
    tok, top = args[0].shape[0], args[2].shape[1]
    heads = args[9].shape[1] // DK
    share = 2 * top * tok // (n_sp * n_tp)
    aligned = share % 16 == 0 and tok // n_tp % 16 == 0 and tok == 128
    if aligned and heads == 1 and args[4].shape[0] == 1 and n_tp == 4 and n_sp & (n_sp - 1) == 0:
        return whole_plan(*args)
    return spread_plan(*args)


def solution(mesh):
    tokens, both = P("sp", None), P("sp", "tp")
    up, down = P("sp", None, "tp"), P("sp", "tp", None)
    return jax.shard_map(
        per_device,
        mesh=mesh,
        in_specs=(tokens,) * 4 + (up, up, down, P(None, "tp")) + (both,) * 5,
        out_specs=(up, up, down) + (both,) * 5,
        check_vma=False,
    )
```

```python
import functools

import jax
import jax.numpy as jnp
from jax import lax
from jax.experimental import pallas as pl
from jax.experimental.pallas import tpu as pltpu
from jax.sharding import PartitionSpec as P

DK = 128
EXACT = lax.Precision.HIGHEST
MESH = pl.DeviceIdType.MESH


def remote(src, dst, send, recv, device):
    return pltpu.make_async_remote_copy(
        src_ref=src, dst_ref=dst, send_sem=send, recv_sem=recv, device_id=device, device_id_type=MESH
    )


def greet(n_sp, me, tp, partners):
    barrier = pltpu.get_barrier_semaphore()

    def hello(i, carry):
        pl.semaphore_signal(
            barrier, inc=1, device_id=(lax.rem(me + i, n_sp), tp), device_id_type=MESH
        )
        return carry

    lax.fori_loop(1, n_sp, hello, 0)
    for other in partners:
        pl.semaphore_signal(barrier, inc=1, device_id=(me, other), device_id_type=MESH)
    pl.semaphore_wait(barrier, n_sp - 1 + len(partners))


def loop(start, stop, body):
    def step(i, carry):
        body(i)
        return carry

    lax.fori_loop(start, stop, step, 0)


def spread_kernel(n_sp, n_tp, n_rows, n_sides, *refs):
    count = n_rows + n_sides
    given, got = refs[:count], refs[count : 2 * count]
    s0, r0, s1, r1, s2, r2, s3, r3, s4, r4, own_sem = refs[2 * count :]
    me, tp = lax.axis_index("sp"), lax.axis_index("tp")
    far = lax.rem(tp + n_tp // 2, n_tp)
    near = tp + 1 - 2 * lax.rem(tp, 2)
    greet(n_sp, me, tp, (far, near))
    rows = tuple(zip(given[:n_rows], got[:n_rows]))
    sides = tuple(zip(given[n_rows:], got[n_rows:]))

    def first(j, p, slot):
        return remote(rows[j][0].at[p], rows[j][1].at[slot, tp], s0.at[j, p], r0.at[j, slot], (p, tp))

    def across(j, p, share):
        ref = rows[j][1].at[p, share]
        return remote(ref, ref, s1.at[j, p], r1.at[j, p], (me, far))

    def beside(j, p, share):
        ref = rows[j][1].at[p, share]
        return remote(ref, ref, s2.at[j, p], r2.at[j, p], (me, near))

    def relay(j, p, share):
        ref = rows[j][1].at[p, share]
        return remote(ref, ref, s3.at[j, p], r3.at[j, p], (me, near))

    def side(k, p, slot):
        return remote(sides[k][0], sides[k][1].at[slot], s4.at[k, p], r4.at[k, slot], (p, tp))

    def send(i):
        p = lax.rem(me + i, n_sp)
        for j in range(n_rows):
            first(j, p, me).start()

    loop(1, n_sp, send)
    owns = [
        pltpu.make_async_copy(rows[j][0].at[me], rows[j][1].at[me, tp], own_sem.at[j]) for j in range(n_rows)
    ] + [pltpu.make_async_copy(sides[k][0], sides[k][1].at[me], own_sem.at[n_rows + k]) for k in range(n_sides)]
    for own in owns:
        own.start()
    for own in owns:
        own.wait()
    for j in range(n_rows):
        across(j, me, tp).start()
        beside(j, me, tp).start()

    def send_side(i):
        p = lax.rem(me + i, n_sp)
        for k in range(n_sides):
            side(k, p, me).start()

    loop(1, n_sp, send_side)

    def forward(i):
        p = lax.rem(me - i + n_sp, n_sp)
        for j in range(n_rows):
            first(j, p, p).wait_recv()
            across(j, p, tp).start()
            beside(j, p, tp).start()

    loop(1, n_sp, forward)

    def pass_on(i):
        p = lax.rem(me - i + n_sp, n_sp)
        for j in range(n_rows):
            across(j, p, far).wait_recv()
            relay(j, p, far).start()

    loop(0, n_sp, pass_on)
    near_far = lax.rem(near + n_tp // 2, n_tp)

    def finish(i):
        p = lax.rem(me - i + n_sp, n_sp)
        for j in range(n_rows):
            beside(j, p, near).wait_recv()
            relay(j, p, near_far).wait_recv()
            across(j, p, tp).wait_send()
            beside(j, p, tp).wait_send()
            relay(j, p, far).wait_send()

    loop(0, n_sp, finish)

    def finish_side(i):
        p = lax.rem(me - i + n_sp, n_sp)
        for k in range(n_sides):
            side(k, p, p).wait_recv()
            side(k, p, me).wait_send()
        for j in range(n_rows):
            first(j, p, me).wait_send()

    loop(1, n_sp, finish_side)


def return_kernel(
    n_sp, n_tp, part, comb, dy, mix, state, mid, gmix, gstate, in1, out1, in2, out2, ret,
    s1, r1, s2, r2, s3, r3, s4, r4, s5, r5, own_sem,
):
    me, tp = lax.axis_index("sp"), lax.axis_index("tp")
    far = lax.rem(tp + n_tp // 2, n_tp)
    near = tp + 1 - 2 * lax.rem(tp, 2)
    near_far = lax.rem(near + n_tp // 2, n_tp)
    quarter = part.shape[2] // n_tp
    greet(n_sp, me, tp, (far, near))

    gathered = ((mix, gmix), (state, gstate))
    strides = [n_sp >> (k + 1) for k in range(n_sp.bit_length() - 1)]

    def hop(j, k, base, c):
        block = lax.rem(base, 2 * strides[k]) + c * 2 * strides[k]
        partner = me + strides[k] * (1 - 2 * lax.rem(me // strides[k], 2))
        ref = gathered[j][1].at[block]
        return remote(ref, ref, s5.at[j, k, c], r5.at[j, block], (partner, tp))

    def widen(k):
        def one(c):
            for j in (0, 1):
                hop(j, k, me, c).start()

        loop(0, n_sp // (2 * strides[k]), one)

    def arrive(k):
        partner = me + strides[k] * (1 - 2 * lax.rem(me // strides[k], 2))

        def one(c):
            for j in (0, 1):
                hop(j, k, partner, c).wait_recv()
                hop(j, k, me, c).wait_send()

        loop(0, n_sp // (2 * strides[k]), one)

    def columns(block):
        return pl.ds(pl.multiple_of(block * quarter, quarter), quarter)

    def beside(j, p):
        block = near if j == 0 else near_far
        return remote(
            part.at[p, :, columns(block)], in1.at[p, j], s1.at[j, p], r1.at[j, p], (me, near)
        )

    def across(p):
        return remote(out1.at[p], in2.at[p], s2.at[p], r2.at[p], (me, far))

    def back(p, slot):
        return remote(out2.at[p], ret.at[slot], s3.at[p], r3.at[slot], (p, tp))

    def start(i):
        p = lax.rem(me + 1 + i, n_sp)
        for j in (1, 0):
            beside(j, p).start()

    loop(0, n_sp, start)
    owns = [
        pltpu.make_async_copy(gathered[j][0], gathered[j][1].at[me], own_sem.at[j]) for j in (0, 1)
    ]
    for own in owns:
        own.start()
    for own in owns:
        own.wait()
    widen(0)

    def pair(i):
        p = lax.rem(me + 1 + i, n_sp)
        beside(1, p).wait_recv()
        mine = part[p, :, columns(far)].astype(jnp.float32)
        out1[p] = (mine + in1[p, 1].astype(jnp.float32)).astype(jnp.bfloat16)
        across(p).start()

    loop(0, n_sp, pair)
    arrive(0)
    for k in range(1, len(strides) - 1):
        widen(k)
        arrive(k)

    def total(p):
        beside(0, p).wait_recv()
        across(p).wait_recv()
        mine = part[p, :, columns(tp)].astype(jnp.float32)
        mine = mine + in1[p, 0].astype(jnp.float32)
        return (mine + in2[p].astype(jnp.float32)).astype(jnp.bfloat16)

    def quad(i):
        p = lax.rem(me + i, n_sp)
        out2[p] = total(p)
        back(p, me).start()

    loop(1, n_sp, quad)
    ret[me] = total(me)
    widen(len(strides) - 1)

    def gather(i, acc):
        p = lax.rem(me - i + n_sp, n_sp)

        @pl.when(i > 0)
        def _():
            back(p, p).wait_recv()

        return acc + jnp.dot(comb[p], ret[p], preferred_element_type=jnp.float32)

    acc = lax.fori_loop(0, n_sp, gather, dy[:, columns(tp)].astype(jnp.float32))
    mid[:, columns(tp)] = acc.astype(jnp.bfloat16)

    def share(k, block, device):
        ref = mid.at[:, columns(block)]
        return remote(ref, ref, s4.at[k], r4.at[k], (me, device))

    share(0, tp, far).start()
    share(1, tp, near).start()
    share(0, far, far).wait_recv()
    share(2, far, near).start()
    share(1, near, near).wait_recv()
    share(2, near_far, near).wait_recv()
    share(0, tp, far).wait_send()
    share(1, tp, near).wait_send()
    share(2, far, near).wait_send()

    arrive(len(strides) - 1)

    def finish(i):
        p = lax.rem(me + i, n_sp)
        for j in (0, 1):
            beside(j, p).wait_send()
        across(p).wait_send()

        @pl.when(i > 0)
        def _():
            back(p, me).wait_send()

    loop(0, n_sp, finish)


VM = pl.BlockSpec(memory_space=pltpu.VMEM)
ANY = pl.BlockSpec(memory_space=pl.ANY)


def dma(*shape):
    return [pltpu.SemaphoreType.DMA(shape), pltpu.SemaphoreType.DMA(shape)]


def call(kernel, ident, operands, in_specs, out_shape, out_specs, scratch):
    return pl.pallas_call(
        kernel,
        out_shape=out_shape,
        in_specs=in_specs,
        out_specs=out_specs,
        scratch_shapes=scratch,
        compiler_params=pltpu.CompilerParams(
            collective_id=ident, has_side_effects=True, vmem_limit_bytes=48 * 1024 * 1024
        ),
    )(*operands)


def spread_plan(
    expert_in, out_cot, route_ids, route_weights, w_gate, w_up, w_down, w_out,
    mixed_heads, queries, keys, values, log_decay,
):
    bf16, f32 = jnp.bfloat16, jnp.float32
    n_sp, n_tp = lax.axis_size("sp"), lax.axis_size("tp")
    me, tp = lax.axis_index("sp"), lax.axis_index("tp")
    tok, width = expert_in.shape
    top = route_ids.shape[1]
    experts = w_gate.shape[0] * n_sp
    cap = 2 * top * tok // experts
    share = cap // n_tp

    ids = route_ids.reshape(-1)
    onehot = ids[:, None] == jnp.arange(experts, dtype=jnp.int32)
    order = jnp.arange(tok * top, dtype=jnp.int32)
    below = (order[None, :] < order[:, None]).astype(bf16)
    ranks = jnp.dot(below, onehot.astype(bf16), preferred_element_type=f32)
    rank = jnp.sum(jnp.where(onehot, ranks, 0.0), axis=1).astype(jnp.int32)
    slot = (ids * cap + rank).reshape(tok, top)
    mine = (
        jnp.arange(experts, dtype=jnp.int32)[:, None] * cap
        + tp * share
        + jnp.arange(share, dtype=jnp.int32)[None, :]
    ).reshape(-1)
    match = slot[None] == mine[:, None, None]
    pick = jnp.any(match, axis=2).astype(bf16)
    slot_weight = jnp.sum(jnp.where(match, route_weights[None], 0.0), axis=(1, 2))
    x_share = jnp.dot(pick, expert_in, preferred_element_type=f32).astype(bf16)
    dy_share = (
        slot_weight[:, None] * jnp.dot(pick, out_cot, preferred_element_type=f32)
    ).astype(bf16)
    places = jnp.arange(experts * cap, dtype=jnp.int32).reshape(experts, 1, cap, 1)
    comb = jnp.any(slot[None, :, None, :] == places, axis=3).astype(bf16)

    heads = queries.shape[1] // DK
    dv = values.shape[1] // heads
    step = jnp.arange(tok, dtype=jnp.int32)
    causal = step[None, :] <= step[:, None]
    lower = causal.astype(f32)
    cumulative = jnp.dot(lower, log_decay, precision=EXACT)
    decay_sum = cumulative[-1:]

    def split(array):
        return array.astype(f32).reshape(tok, heads, -1)

    q, k, v = split(queries), split(keys), split(values)
    grow, shrink, to_end = (
        split(jnp.exp(-cumulative)),
        split(jnp.exp(cumulative)),
        split(jnp.exp(decay_sum - cumulative)),
    )
    qd, kg, ke = q * shrink, k * grow, k * to_end
    state_local = jnp.einsum("thd,the->hde", ke, v, precision=EXACT)

    rows = jax.ShapeDtypeStruct((n_sp, n_tp, share, width), bf16)
    gx, gdy, gdecay = call(
        functools.partial(spread_kernel, n_sp, n_tp, 2, 1),
        0,
        (
            x_share.reshape(n_sp, share, width),
            dy_share.reshape(n_sp, share, width),
            decay_sum,
        ),
        [VM] * 3,
        (
            rows,
            rows,
            jax.ShapeDtypeStruct((n_sp,) + decay_sum.shape, f32),
        ),
        (ANY, ANY, ANY),
        dma(2, n_sp) * 4 + dma(1, n_sp) + [pltpu.SemaphoreType.DMA((3,))],
    )
    got_x = gx.reshape(n_sp * cap, width)
    got_dy = gdy.reshape(n_sp * cap, width)
    wg, wu, wd = w_gate[0], w_up[0], w_down[0]
    gate_pre = jnp.dot(got_x, wg, preferred_element_type=f32)
    up_pre = jnp.dot(got_x, wu, preferred_element_type=f32)
    hidden_cot = lax.dot_general(got_dy, wd, (((1,), (1,)), ((), ())), preferred_element_type=f32)
    sig = jax.nn.sigmoid(gate_pre)
    hidden = (gate_pre * sig * up_pre).astype(bf16)
    gate_cot = (hidden_cot * up_pre * sig * (1.0 + gate_pre * (1.0 - sig))).astype(bf16)
    up_cot = (hidden_cot * gate_pre * sig).astype(bf16)
    back = (((1,), (1,)), ((), ()))
    part = lax.dot_general(gate_cot, wg, back, preferred_element_type=f32) + lax.dot_general(
        up_cot, wu, back, preferred_element_type=f32
    )
    part = part.astype(bf16).reshape(n_sp, cap, width)
    over = (((0,), (0,)), ((), ()))
    grad_gate = lax.dot_general(got_x, gate_cot, over, preferred_element_type=f32)[None]
    grad_up = lax.dot_general(got_x, up_cot, over, preferred_element_type=f32)[None]
    grad_down = lax.dot_general(hidden, got_dy, over, preferred_element_type=f32)[None]

    quarter = width // n_tp
    buf = pltpu.VMEM((n_sp, cap, quarter), bf16)
    mid, gmix, gstate = call(
        functools.partial(return_kernel, n_sp, n_tp),
        1,
        (part, comb, out_cot, mixed_heads, state_local.reshape(heads * DK, dv).astype(bf16)),
        [VM] * 5,
        (
            jax.ShapeDtypeStruct((tok, width), bf16),
            jax.ShapeDtypeStruct((n_sp,) + mixed_heads.shape, bf16),
            jax.ShapeDtypeStruct((n_sp, heads * DK, dv), bf16),
        ),
        (VM, VM, VM),
        [pltpu.VMEM((n_sp, 2, cap, quarter), bf16), buf, buf, buf, buf]
        + dma(2, n_sp) + dma(n_sp) + dma(n_sp) + dma(3)
        + [
            pltpu.SemaphoreType.DMA((2, n_sp.bit_length() - 1, n_sp // 2)),
            pltpu.SemaphoreType.DMA((2, n_sp)),
            pltpu.SemaphoreType.DMA((2,)),
        ],
    )
    head_cot = split(jnp.dot(mid, w_out, preferred_element_type=f32))
    pull = jnp.einsum("thd,the->hde", qd, head_cot, precision=EXACT)
    part_tok = tok // n_tp
    cols = lax.dynamic_slice_in_dim(mid, tp * part_tok, part_tok, 0)
    cols = cols.reshape(part_tok, n_sp, width // n_sp).swapaxes(0, 1)
    gcols, gpull = call(
        functools.partial(spread_kernel, n_sp, n_tp, 1, 1),
        2,
        (cols, pull.reshape(heads * DK, dv).astype(bf16)),
        [VM] * 2,
        (
            jax.ShapeDtypeStruct((n_sp, n_tp, part_tok, width // n_sp), bf16),
            jax.ShapeDtypeStruct((n_sp, heads * DK, dv), bf16),
        ),
        (VM, VM),
        dma(1, n_sp) * 5 + [pltpu.SemaphoreType.DMA((2,))],
    )
    gcols = gcols.reshape(n_sp, tok, width // n_sp)
    grad_out_proj = jnp.einsum("ntd,nte->de", gcols, gmix, preferred_element_type=f32)

    sums = gdecay[:, 0]
    index = jnp.arange(n_sp, dtype=jnp.int32)
    between = (index[None] > jnp.minimum(index, me)[:, None]) & (
        index[None] < jnp.maximum(index, me)[:, None]
    )
    weight = jnp.exp(jnp.sum(jnp.where(between[..., None], sums[None], 0.0), axis=1))

    def entering(pieces, used):
        scale = jnp.where(used[:, None], weight, 0.0)
        return jnp.sum(scale[..., None] * pieces.astype(f32), axis=0).reshape(heads, DK, dv)

    state_in = entering(gstate, index < me)
    state_cot = entering(gpull, index > me)

    dot = functools.partial(jnp.einsum, precision=EXACT)
    scores = jnp.where(causal, dot("thd,shd->hts", qd, kg), 0.0)
    scores_cot = jnp.where(causal, dot("the,she->hts", head_cot, v), 0.0)
    grad_v = dot("hts,the->she", scores, head_cot) + dot("shd,hde->she", ke, state_cot)
    qd_cot = dot("hts,shd->thd", scores_cot, kg) + dot("the,hde->thd", head_cot, state_in)
    kg_cot = dot("hts,thd->shd", scores_cot, qd)
    ke_cot = dot("she,hde->shd", v, state_cot)
    end = ke_cot * ke
    c_cot = (qd_cot * qd - kg_cot * kg - end).reshape(tok, heads * DK)
    last = jnp.sum(end, axis=0).reshape(-1) + jnp.exp(decay_sum[0]) * jnp.sum(
        state_cot * state_in, axis=2
    ).reshape(-1)
    grad_decay = lax.dot_general(lower, c_cot, over, precision=EXACT) + last[None]
    grad_q = (qd_cot * shrink).astype(bf16).reshape(tok, heads * DK)
    grad_k = (kg_cot * grow + ke_cot * to_end).astype(bf16).reshape(tok, heads * DK)
    return (
        grad_gate,
        grad_up,
        grad_down,
        grad_out_proj,
        grad_q,
        grad_k,
        grad_v.astype(bf16).reshape(tok, heads * dv),
        grad_decay,
    )


class Copies:
    def __init__(self, send, recv):
        self.send, self.recv = send, recv


def dot(a, b, dims, exact=False):
    return lax.dot_general(
        a, b, (dims, ((), ())), precision=EXACT if exact else None, preferred_element_type=jnp.float32
    )


NN, NT, TN = ((1,), (0,)), ((1,), (1,)), ((0,), (0,))


def whole_kernel(n_sp, n_tp, *refs):
    bf16, f32 = jnp.bfloat16, jnp.float32
    given, refs = refs[:13], refs[13:]
    outs, refs = refs[:8], refs[8:]
    x_hbm, dy_hbm, ids, weights, *_ = given
    out_gate, out_up, out_down, grad_proj, grad_q, grad_k, grad_v, grad_decay = outs
    (
        x_in, dy_in, wg, wu, wd, wo, mixed, qv, kv, vv, gv,
        pos_t, wt, comb, xs, dys, gx, gdy, cots, hid, part, in1, out1, in2, out2, ret,
        mid, gmix, gcols, dall, fsend, frecv, usend, urecv, ftot, fpre, utot, upre,
        head, qd_s, kg_s, ke_s, sc_s, qc_s, kc_s, gv_s, cum_s,
        grad_gate, grad_up, grad_down, load, own_sem, put_sem, *sems,
    ) = refs
    pairs = [Copies(a, b) for a, b in zip(sems[::2], sems[1::2])]
    (
        c_first, c_across, c_beside, c_relay, c_sum, c_mix, c_fwd, c_half, c_cross, c_back,
        c_share, c_rev, d_first, d_across, d_beside, d_relay,
    ) = pairs
    me, tp = lax.axis_index("sp"), lax.axis_index("tp")
    far = lax.rem(tp + n_tp // 2, n_tp)
    near = tp + 1 - 2 * lax.rem(tp, 2)
    near_far = lax.rem(near + n_tp // 2, n_tp)
    tok, width = x_in.shape
    share = xs.shape[1]
    cap = share * n_tp
    quarter = width // n_tp
    piece = width // n_sp
    rows = tok // n_tp
    bits = n_sp.bit_length() - 1

    sources = (x_hbm, dy_hbm) + tuple(given[4:])
    places = (x_in, dy_in, wg, wu, wd, wo, mixed, qv, kv, vv, gv)

    def fetch(i):
        src = sources[i].at[0] if len(sources[i].shape) == 3 else sources[i]
        return pltpu.make_async_copy(src, places[i], load.at[i])

    for i in range(len(places)):
        fetch(i).start()

    barrier = pltpu.get_barrier_semaphore()

    def hello(i):
        pl.semaphore_signal(
            barrier, inc=1, device_id=(lax.rem(me + i, n_sp), tp), device_id_type=MESH
        )

    loop(1, n_sp, hello)
    for other in (far, near):
        pl.semaphore_signal(barrier, inc=1, device_id=(me, other), device_id_type=MESH)

    def flip(m):
        out = 0
        for b in range(bits):
            a, c = lax.rem(me // (1 << b), 2), lax.rem(m // (1 << b), 2)
            out = out + (1 << b) * (a + c - 2 * a * c)
        return out

    def turn(i):
        zero = 1 - (i + n_sp - 1) // n_sp
        is_near = lax.rem(i, 2) * (1 - i // (n_sp - 1)) + zero
        half_way = (i + 1) // 2
        return half_way + (1 - is_near) * (n_sp // 2 - 1)

    def peer(i):
        return flip(turn(i))

    others = pl.ds(0, n_sp - 1)

    def whole(copies, ref):
        recv = copies.recv.at[(0,) * len(copies.recv.shape)] if copies.recv.shape else copies.recv
        return remote(ref, ref, copies.send, recv, (me, far))

    def got_all(copies, ref):
        whole(copies, ref).wait_recv()

    def columns(block):
        return pl.ds(pl.multiple_of(block * quarter, quarter), quarter)

    down = lax.broadcasted_iota(jnp.int32, (tok, tok), 0)
    across_i = lax.broadcasted_iota(jnp.int32, (tok, tok), 1)
    weight, hit = jnp.zeros((tok, tok), f32), jnp.zeros((tok, tok), f32)
    for j in range(ids.shape[0]):
        hit_j = ids[j : j + 1, :] == down
        weight = weight + jnp.where(hit_j, weights[j : j + 1, :], 0.0)
        hit = hit + jnp.where(hit_j, 1.0, 0.0)
    above = jnp.where(down < across_i, 1.0, 0.0).astype(bf16)
    pos = jnp.where(hit > 0.5, dot(hit.astype(bf16), above, NN), -1.0)
    pos_t[...] = pos
    wt[...] = weight
    pos = jnp.transpose(pos)
    slot_lane = lax.broadcasted_iota(jnp.int32, (tok, cap), 1).astype(f32)
    for e in range(n_sp):
        comb[:, e * cap : (e + 1) * cap] = jnp.where(pos[:, e : e + 1] == slot_lane, 1.0, 0.0).astype(bf16)

    fetch(0).wait()
    fetch(1).wait()

    def chosen(e, start, count):
        want = (lax.broadcasted_iota(jnp.int32, (count, tok), 0) + start).astype(f32)
        match = pos_t[pl.ds(e, 1), :] == want
        scale = jnp.sum(jnp.where(match, wt[pl.ds(e, 1), :], 0.0), axis=1, keepdims=True)
        return jnp.where(match, 1.0, 0.0), scale

    found = [chosen(e, tp * share, share) for e in range(n_sp)]
    pick = jnp.concatenate([a for a, _ in found], axis=0).astype(bf16)
    scale = jnp.concatenate([b for _, b in found], axis=0)
    xs[...] = dot(pick, x_in[...], NN).astype(bf16).reshape(n_sp, share, width)
    dys[...] = (scale * dot(pick, dy_in[...], NN)).astype(bf16).reshape(n_sp, share, width)

    pl.semaphore_wait(barrier, n_sp + 1)

    row_pairs = ((xs, gx), (dys, gdy))

    def first(j, p, slot):
        return remote(
            row_pairs[j][0].at[p], row_pairs[j][1].at[slot, tp],
            c_first.send, c_first.recv.at[j, slot], (p, tp),
        )

    def passing(copies, j, p, block, device):
        ref = row_pairs[j][1].at[p, block]
        return remote(ref, ref, copies.send, copies.recv.at[p], (me, device))

    def arrived(copies, p):
        ref = gx.at[p, pl.ds(0, 2)]
        remote(ref, ref, copies.send, copies.recv.at[p], (me, far)).wait_recv()

    def across(j, p, block):
        return passing(c_across, j, p, block, far)

    def beside(j, p, block):
        return passing(c_beside, j, p, block, near)

    def relay(j, p, block):
        return passing(c_relay, j, p, block, near)

    def dispatch(m):
        p = peer(m)
        for j in (0, 1):
            first(j, p, me).start()

    loop(1, n_sp, dispatch)

    own_pick, own_scale = chosen(me, 0, cap)
    own_pick = own_pick.astype(bf16)
    gx[me] = dot(own_pick, x_in[...], NN).astype(bf16).reshape(n_tp, share, width)
    gdy[me] = (own_scale * dot(own_pick, dy_in[...], NN)).astype(bf16).reshape(n_tp, share, width)

    for i in range(6, 11):
        fetch(i).wait()
    causal = across_i <= down
    lower = jnp.where(causal, 1.0, 0.0)
    cum = dot(lower, gv[...], NN, True)
    total_decay = cum[tok - 1 : tok, :]
    cum_s[...] = cum
    dall[me] = jnp.broadcast_to(total_decay, dall.shape[1:])

    def decay(p, slot):
        return remote(dall.at[me], dall.at[slot], c_sum.send, c_sum.recv, (p, tp))

    def send_decay(m):
        decay(flip(m), me).start()

    loop(1, n_sp, send_decay)
    key = kv[...].astype(f32)
    val = vv[...].astype(f32)
    qd_s[...] = qv[...].astype(f32) * jnp.exp(cum)
    kg_s[...] = key * jnp.exp(-cum)
    ke_s[...] = key * jnp.exp(total_decay - cum)
    ftot[...] = dot(val, ke_s[...], TN, True)
    fpre[...] = jnp.zeros_like(fpre)

    piece_rows = ftot.shape[0] // 2
    is_low, is_high = me < n_sp // 2, me >= n_sp // 2

    def hop(copies, held, got, k, c):
        partner = me + (1 << k) * (1 - 2 * lax.rem(me // (1 << k), 2))
        return remote(held.at[k, c], got.at[k, c], copies.send, copies.recv.at[k, c], (partner, tp))

    def lines(c):
        return slice(c * piece_rows, (c + 1) * piece_rows)

    def give(copies, held, got, total, k, c):
        held[k, c] = total[lines(c), :].astype(bf16)
        if k < bits - 1:
            hop(copies, held, got, k, c).start()
        else:

            @pl.when(is_low if copies is c_fwd else is_high)
            def _():
                hop(copies, held, got, k, c).start()

    def decay_over(low, high):
        table = dall[:, 0, :]
        index = lax.broadcasted_iota(jnp.int32, table.shape, 0)
        picked = jnp.where((index >= low) & (index < high), table, 0.0)
        return jnp.exp(jnp.sum(picked, axis=0, keepdims=True))

    def span(k):
        size = 1 << k
        base = me - lax.rem(me, size)
        upper = lax.rem(me // size, 2)
        return base, base + size, upper

    def forward_merge(k, c):
        hop(c_fwd, fsend, frecv, k, c).wait_recv()
        low, high, upper = span(k)
        got = frecv[k, c].astype(f32)
        is_upper = upper == 1
        at = lines(c)
        fpre[at, :] = fpre[at, :] + jnp.where(is_upper, decay_over(low, me), 0.0) * got
        mine = jnp.where(is_upper, 1.0, decay_over(low + (1 << k), high + (1 << k)))
        theirs = jnp.where(is_upper, decay_over(low, high), 1.0)
        if k < bits - 1:
            ftot[at, :] = mine * ftot[at, :] + theirs * got

    def reverse_merge(k, c):
        low, high, upper = span(k)
        is_upper = upper == 1
        after = jnp.where(is_upper, 0.0, decay_over(me + 1, high))
        mine = jnp.where(is_upper, decay_over(low - (1 << k), low), 1.0)
        theirs = jnp.where(is_upper, 1.0, decay_over(low, high))
        hop(c_rev, usend, urecv, k, c).wait_recv()
        got = urecv[k, c].astype(f32)
        at = lines(c)
        if k < bits - 1:
            utot[at, :] = mine * utot[at, :] + theirs * got
            give(c_rev, usend, urecv, utot, k + 1, c)
        upre[at, :] = upre[at, :] + after * got

    strides = [n_sp >> (k + 1) for k in range(bits)]

    def mix_hop(k, base, c):
        block = lax.rem(base, 2 * strides[k]) + c * 2 * strides[k]
        block = lax.rem(block, n_sp)
        partner = me + strides[k] * (1 - 2 * lax.rem(me // strides[k], 2))
        ref = gmix.at[block]
        return remote(ref, ref, c_mix.send, c_mix.recv.at[block], (partner, tp))

    def widen(k):
        def one(c):
            mix_hop(k, me, c).start()

        loop(0, n_sp // (2 * strides[k]), one)

    def arrive(k):
        partner = me + strides[k] * (1 - 2 * lax.rem(me // strides[k], 2))

        def one(c):
            mix_hop(k, partner, c).wait_recv()

        loop(0, n_sp // (2 * strides[k]), one)

    own_mix = pltpu.make_async_copy(mixed, gmix.at[me], own_sem)
    own_mix.start()
    own_mix.wait()
    widen(0)
    for c in (0, 1):
        give(c_fwd, fsend, frecv, ftot, 0, c)
    sc_s[...] = jnp.where(causal, dot(qd_s[...], kg_s[...], NT, True), 0.0)
    for i in range(2, 6):
        fetch(i).wait()

    def half(j, p):
        block = near if j == 0 else near_far
        return remote(
            part.at[p, :, columns(block)], in1.at[p, j], c_half.send, c_half.recv.at[j, p], (me, near)
        )

    def cross(p):
        return remote(out1.at[p], in2.at[p], c_cross.send, c_cross.recv.at[p], (me, far))

    def back(p, slot):
        return remote(out2.at[p], ret.at[slot], c_back.send, c_back.recv, (p, tp))

    def expert(m):
        p = peer(m)

        @pl.when(m > 0)
        def _():
            arrived(c_beside, p)
            arrived(c_relay, p)

        x = gx[p].reshape(cap, width)
        dy = gdy[p].reshape(cap, width)
        gate = dot(x, wg[...], NN)
        up = dot(x, wu[...], NN)
        hidden_cot = dot(dy, wd[...], NT)
        sig = jax.nn.sigmoid(gate)
        hid[p] = (gate * sig * up).astype(bf16)
        gate_cot = (hidden_cot * up * sig * (1.0 + gate * (1.0 - sig))).astype(bf16)
        up_cot = (hidden_cot * gate * sig).astype(bf16)
        units = gate_cot.shape[1]
        cots[p, :, :units] = gate_cot
        cots[p, :, units:] = up_cot
        part[p] = (dot(gate_cot, wg[...], NT) + dot(up_cot, wu[...], NT)).astype(bf16)
        for j in (1, 0):
            half(j, p).start()

    def step(i):
        @pl.when((i >= 3) & (i < n_sp + 3))
        def _():
            p = peer(i - 3)
            half(1, p).wait_recv()
            mine = part[p, :, columns(far)].astype(f32)
            out1[p] = (mine + in1[p, 1].astype(f32)).astype(bf16)
            cross(p).start()

        @pl.when(i < n_sp)
        def _():
            p = peer(i)
            for j in (0, 1):
                first(j, p, p).wait_recv()
                across(j, p, tp).start()
                beside(j, p, tp).start()

        @pl.when((i >= 3) & (i < n_sp + 2))
        def _():
            expert(i - 2)

        @pl.when((i >= 2) & (i < n_sp + 1))
        def _():
            p = peer(i - 1)
            arrived(c_across, p)
            for j in (0, 1):
                relay(j, p, far).start()

        @pl.when(i >= 4)
        def _():
            p = peer(i - 4)
            half(0, p).wait_recv()
            cross(p).wait_recv()
            mine = part[p, :, columns(tp)].astype(f32)
            mine = mine + in1[p, 0].astype(f32)
            out2[p] = (mine + in2[p].astype(f32)).astype(bf16)

            @pl.when(i > 4)
            def _():
                back(p, me).start()

    expert(0)
    loop(1, n_sp, step)
    arrive(0)
    widen(1)
    loop(n_sp, n_sp + 2, step)
    for n in range(1, bits - 1):
        arrive(n)
        widen(n + 1)
    loop(n_sp + 2, n_sp + 4, step)
    ret[me] = out2[me]

    all_x = gx.reshape(n_sp * cap, width)
    all_dy = gdy.reshape(n_sp * cap, width)
    tile = 256

    def weight_grad(b):
        at = pl.ds(pl.multiple_of(b * tile, tile), tile)
        both = cots[...].reshape(n_sp * cap, cots.shape[2])
        units = cots.shape[2] // 2
        grads = dot(all_x[:, at], both, TN)
        grad_gate[at, :] = grads[:, :units]
        grad_up[at, :] = grads[:, units:]

    def down_grad(b):
        at = pl.ds(pl.multiple_of(b * tile, tile), tile)
        grad_down[:, at] = dot(hid[...].reshape(n_sp * cap, hid.shape[2]), all_dy[:, at], TN)

    def put(i):
        src = (grad_gate, grad_up, grad_down)[i]
        return pltpu.make_async_copy(src, (out_gate, out_up, out_down)[i], put_sem.at[i])

    loop(0, width // tile, down_grad)
    put(2).start()
    got_all(c_back, ret.at[others])
    acc = dot(comb[...], ret[...].reshape(n_sp * cap, quarter), NN)
    mid[:, columns(tp)] = (acc + dy_in[:, columns(tp)].astype(f32)).astype(bf16)

    def spread(k, block, device):
        ref = mid.at[:, columns(block)]
        return remote(ref, ref, c_share.send, c_share.recv.at[k], (me, device))

    def project(block):
        at = pl.ds(pl.multiple_of(block * quarter, quarter), quarter)
        return dot(mid[:, columns(block)], wo[at, :], NN)

    spread(0, tp, far).start()
    spread(1, tp, near).start()
    got_all(c_sum, dall.at[others])
    for c in (0, 1):
        forward_merge(0, c)
        give(c_fwd, fsend, frecv, ftot, 1, c)
    head[...] = project(tp)
    spread(1, near, near).wait_recv()
    head[...] += project(near)
    spread(0, far, far).wait_recv()
    spread(2, far, near).start()
    head[...] += project(far)
    spread(2, near_far, near).wait_recv()
    head[...] += project(near_far)

    utot[...] = dot(head[...], qd_s[...], TN, True)
    upre[...] = jnp.zeros_like(upre)
    for c in (0, 1):
        give(c_rev, usend, urecv, utot, 0, c)

    def col_first(p, slot):
        at = pl.ds(pl.multiple_of(p * piece, piece), piece)
        mine = pl.ds(pl.multiple_of(tp * rows, rows), rows)
        return remote(
            mid.at[mine, at], gcols.at[slot, tp], d_first.send, d_first.recv, (p, tp)
        )

    def col_pass(copies, p, block, device):
        ref = gcols.at[p, block]
        return remote(ref, ref, copies.send, copies.recv, (me, device))

    def send_cols(m):
        col_first(flip(m), me).start()

    loop(1, n_sp, send_cols)
    own_at = pl.ds(pl.multiple_of(me * piece, piece), piece)
    gcols[me] = mid[:, own_at].reshape(n_tp, rows, piece)
    scores_cot = jnp.where(causal, dot(head[...], vv[...].astype(f32), NT, True), 0.0)
    for k in range(1, bits - 1):
        for c in (0, 1):
            forward_merge(k, c)
            give(c_fwd, fsend, frecv, ftot, k + 1, c)
    qc_s[...] = dot(scores_cot, kg_s[...], NN, True)
    kc_s[...] = dot(scores_cot, qd_s[...], TN, True)
    gv_s[...] = dot(sc_s[...], head[...], TN, True)

    def col_forward():
        got_all(d_first, gcols.at[others, 0])

        def one(m):
            p = flip(m)
            col_pass(d_across, p, tp, far).start()
            col_pass(d_beside, p, tp, near).start()

        loop(1, n_sp, one)

    def col_relay():
        got_all(d_across, gcols.at[others, 0])

        def one(m):
            col_pass(d_relay, flip(m), far, near).start()

        loop(1, n_sp, one)

    steps = width // tile
    for k in range(bits - 1):
        loop(steps * k // (bits - 1), steps * (k + 1) // (bits - 1), weight_grad)
        if k == bits - 2:
            put(0).start()
            put(1).start()
            pl.when(me < n_sp // 2)(col_forward)
        for c in (0, 1):
            reverse_merge(k, c)
    pl.when(me >= n_sp // 2)(col_forward)
    col_relay()

    @pl.when(is_low)
    def _():
        for c in (0, 1):
            reverse_merge(bits - 1, c)

    @pl.when(is_high)
    def _():
        for c in (0, 1):
            forward_merge(bits - 1, c)

    carry, enter = upre[...], fpre[...]
    qc_s[...] += dot(head[...], enter, NN, True)
    cum = cum_s[...]
    total_decay = cum[tok - 1 : tok, :]
    val = vv[...].astype(f32)
    ke_cot = dot(val, carry, NN, True)
    grad_v[...] = (gv_s[...] + dot(ke_s[...], carry, NT, True)).astype(bf16)
    end = ke_cot * ke_s[...]
    c_cot = qc_s[...] * qd_s[...] - kc_s[...] * kg_s[...] - end
    last = jnp.sum(end, axis=0, keepdims=True) + jnp.exp(total_decay) * jnp.sum(
        carry * enter, axis=0, keepdims=True
    )
    grad_decay[...] = dot(lower, c_cot, TN, True) + last
    grad_q[...] = (qc_s[...] * jnp.exp(cum)).astype(bf16)
    grad_k[...] = (kc_s[...] * jnp.exp(-cum) + ke_cot * jnp.exp(total_decay - cum)).astype(bf16)

    arrive(bits - 1)

    got_all(d_beside, gcols.at[others, 0])
    got_all(d_relay, gcols.at[others, 0])
    grad_proj[...] = dot(
        gcols[...].reshape(n_sp * tok, piece), gmix[...].reshape(n_sp * tok, gmix.shape[2]), TN
    )

    def sent(copies, ref):
        whole(copies, ref).wait_send()

    for copies in (c_first, c_across, c_beside, c_relay):
        sent(copies, gx.at[others, pl.ds(0, 2)])
    for copies in (d_first, d_across, d_beside, d_relay):
        sent(copies, gcols.at[others, 0])
    sent(c_sum, dall.at[others])
    sent(c_mix, gmix.at[others])

    @pl.when(is_low)
    def _():
        sent(c_fwd, fsend)
        sent(c_rev, usend.at[pl.ds(0, bits - 1)])

    @pl.when(is_high)
    def _():
        sent(c_fwd, fsend.at[pl.ds(0, bits - 1)])
        sent(c_rev, usend)

    sent(c_half, in1)
    sent(c_cross, out1)
    sent(c_back, out2.at[others])
    sent(c_share, mid.at[:, pl.ds(0, 3 * quarter)])
    for i in range(3):
        put(i).wait()


def flush_kernel(*refs):
    count = (len(refs) - 1) // 2
    copies = [
        pltpu.make_async_copy(refs[i], refs[count + i], refs[-1].at[i]) for i in range(count)
    ]
    for copy in copies:
        copy.start()
    for copy in copies:
        copy.wait()


def flush(arrays):
    count = len(arrays)
    return pl.pallas_call(
        flush_kernel,
        out_shape=tuple(jax.ShapeDtypeStruct(a.shape, a.dtype) for a in arrays),
        in_specs=[VM] * count,
        out_specs=(ANY,) * count,
        scratch_shapes=[pltpu.SemaphoreType.DMA((count,))],
        compiler_params=pltpu.CompilerParams(vmem_limit_bytes=1024 * 1024),
    )(*[pltpu.with_memory_space_constraint(a, pltpu.VMEM) for a in arrays])


def whole_plan(*args):
    bf16, f32 = jnp.bfloat16, jnp.float32
    n_sp, n_tp = lax.axis_size("sp"), lax.axis_size("tp")
    expert_in, route_ids, w_gate = args[0], args[2], args[4]
    tok, width = expert_in.shape
    units = w_gate.shape[2]
    cap = 2 * route_ids.shape[1] * tok // n_sp
    share, quarter, piece = cap // n_tp, width // n_tp, width // n_sp
    dv = args[11].shape[1]
    bits = n_sp.bit_length() - 1
    mem = pltpu.VMEM
    held = [
        mem(a.shape[1:] if a.ndim == 3 else a.shape, a.dtype) for a in args[:2] + args[4:]
    ]
    state = (dv, DK)
    scratch = held + [
        mem((tok, tok), f32), mem((tok, tok), f32), mem((tok, n_sp * cap), bf16),
        mem((n_sp, share, width), bf16), mem((n_sp, share, width), bf16),
        mem((n_sp, n_tp, share, width), bf16), mem((n_sp, n_tp, share, width), bf16),
        mem((n_sp, cap, 2 * units), bf16), mem((n_sp, cap, units), bf16), mem((n_sp, cap, width), bf16),
        mem((n_sp, 2, cap, quarter), bf16),
    ] + [mem((n_sp, cap, quarter), bf16)] * 4 + [
        mem((tok, width), bf16), mem((n_sp,) + args[8].shape, bf16), mem((n_sp, n_tp, tok // n_tp, piece), bf16),
        mem((n_sp, 8, DK), f32),
    ] + [mem((bits, 2, dv // 2, DK), bf16)] * 4 + [mem(state, f32)] * 4 + [mem((tok, dv), f32)] + [
        mem((tok, DK), f32)
    ] * 3 + [mem((tok, tok), f32), mem((tok, DK), f32), mem((tok, DK), f32), mem((tok, dv), f32), mem((tok, DK), f32)]
    scratch += [mem((width, units), f32)] * 2 + [mem((units, width), f32)]
    scratch += [pltpu.SemaphoreType.DMA((11,)), pltpu.SemaphoreType.DMA, pltpu.SemaphoreType.DMA((3,))]
    one = pltpu.SemaphoreType.DMA
    counts = [(2, n_sp)] + [(n_sp,)] * 3 + [(), (n_sp,)] + [(bits, 2), (2, n_sp), (n_sp,), (), (3,), (bits, 2)] + [()] * 4
    for count in counts:
        scratch += [one, one(count) if count else one]
    shapes = [
        ((width, units), f32), ((width, units), f32), ((units, width), f32), ((piece, args[8].shape[1]), f32),
        (args[9].shape, bf16), (args[10].shape, bf16), (args[11].shape, bf16), (args[12].shape, f32),
    ]
    outs = pl.pallas_call(
        functools.partial(whole_kernel, n_sp, n_tp),
        out_shape=tuple(pltpu.VMEM(s, t) for s, t in shapes),
        in_specs=[ANY, ANY, VM, VM] + [ANY] * 9,
        out_specs=(ANY,) * 3 + (VM,) * 5,
        scratch_shapes=scratch,
        compiler_params=pltpu.CompilerParams(
            collective_id=3, has_side_effects=True, vmem_limit_bytes=56 * 1024 * 1024
        ),
    )(*args[:2], args[2].T, args[3].T, *args[4:])
    outs = flush(outs)
    return tuple(a[None] for a in outs[:3]) + tuple(outs[3:])


def per_device(*args):
    n_sp, n_tp = lax.axis_size("sp"), lax.axis_size("tp")
    tok, top = args[0].shape[0], args[2].shape[1]
    heads = args[9].shape[1] // DK
    share = 2 * top * tok // (n_sp * n_tp)
    aligned = share % 16 == 0 and tok // n_tp % 16 == 0 and tok == 128
    if aligned and heads == 1 and args[4].shape[0] == 1 and n_tp == 4 and n_sp & (n_sp - 1) == 0:
        return whole_plan(*args)
    return spread_plan(*args)


def solution(mesh):
    tokens, both = P("sp", None), P("sp", "tp")
    up, down = P("sp", None, "tp"), P("sp", "tp", None)
    return jax.shard_map(
        per_device,
        mesh=mesh,
        in_specs=(tokens,) * 4 + (up, up, down, P(None, "tp")) + (both,) * 5,
        out_specs=(up, up, down) + (both,) * 5,
        check_vma=False,
    )
```
